256 devices in a mesh: ep: 16 (over y, x), tp: 16 (over z, core).
Axes of the slice: x: 4, y: 4, z: 8, core: 2. Of those that a mesh axis runs over, the one named last changes fastest.
Arguments:
- receptance: bfloat16 [32768, 1024], P('ep', 'tp'), may hold values from -6 to 6
- key_in: bfloat16 [32768, 1024], P('ep', 'tp'), may hold values from -6 to 6
- payload_vectors: bfloat16 [32768, 1024], P('ep', 'tp'), may hold values from -6 to 6
- decay_in: bfloat16 [32768, 1024], P('ep', 'tp'), may hold values from -30 to 3
- rate_in: bfloat16 [32768, 1024], P('ep', 'tp'), may hold values from -30 to 6
- gate_in: bfloat16 [32768, 1024], P('ep', 'tp'), may hold values from -6 to 6
- norm_gain: float32 [1024], P('tp'), may hold values from 0.1 to 1.9
- out_weight: bfloat16 [1024, 2048], P('tp'), may hold values from -0.1875 to 0.1875
- moe_in: bfloat16 [32768, 2048], P(('ep', 'tp')), may hold values from -6 to 6
- moe_gain: float32 [2048], replicated, may hold values from 0.1 to 1.9
- routes: int32 [32768, 2], P(('ep', 'tp')), may hold values from 0 to 31, all different within a row; in each aligned block of 128 rows (0 to 127, 128 to 255, ...) at most 12 rows name the same one
- route_weights: float32 [32768, 2], P(('ep', 'tp')), may hold values from 0.2 to 1
- expert_gate: bfloat16 [32, 2048, 512], P('ep', None, 'tp'), may hold values from -0.125 to 0.125
- expert_up: bfloat16 [32, 2048, 512], P('ep', None, 'tp'), may hold values from -0.125 to 0.125
- expert_down: bfloat16 [32, 2048, 512], P('ep', None, 'tp'), may hold values from -0.25 to 0.25
- shared_gate: bfloat16 [2048, 512], replicated, may hold values from -0.125 to 0.125
- shared_up: bfloat16 [2048, 512], replicated, may hold values from -0.125 to 0.125
- shared_down: bfloat16 [512, 2048], replicated, may hold values from -0.25 to 0.25
Outputs:
- mixed: bfloat16 [32768, 2048], P(('ep', 'tp'))
- moe_out: bfloat16 [32768, 2048], P(('ep', 'tp'))
The draws below stay inside these ranges and needn't reach their ends.
Inputs may be any that keep to these rules, and one draw needn't show every extreme that they name: `routes`: each token names 2 different experts; within the rows of one device no expert is named more than 12 times, a bound that some block reaches there.
All inputs are finite; a program needn't handle non-finite values.
Results may differ from the reference program's by a relative error of at most 0.019.
Values may be sent and summed in bfloat16 or wider, within the bound.
No kernel may reach another device: no remote copies, remote signals or barrier semaphores. Data moves between devices by JAX's collectives and lax.ppermute only.
A program may use at most 128 MiB of HBM per device.

```python
import math
import jax
import jax.numpy as jnp
import numpy as np
from jax import lax

D = 2048
MIX_WIDTH = 1024
HEAD_DIM = 64
HEADS = 16
BLOCK = 64
SEQ = 32768
MOE_TOKENS = 128
MOE_ALL = 32768
TOP_K = 2
EXPERTS = 32
EXPERT_WIDTH = 512
SHARED_WIDTH = 512
SLOTS = 12


def slow_channel_index(key):
    kinds = jax.random.randint(jax.random.fold_in(key, 11), (HEADS,), 0, 8)
    slow = kinds < 4
    return jnp.repeat(slow, HEAD_DIM)[None, :]


def draw_decay_in(key, part):
    slow = slow_channel_index(key)
    capacity_locations = jnp.arange(SEQ, dtype=jnp.int32)
    noise = jnp.clip(jax.random.normal(jax.random.fold_in(key, 1), (SEQ, MIX_WIDTH), jnp.float32), -2.0, 2.0) * 0.7
    spans = jax.random.uniform(jax.random.fold_in(key, 2), (16,), jnp.float32, -0.7, 0.7)
    shift = spans[capacity_locations * 16 // SEQ][:, None]
    channel = jax.random.uniform(jax.random.fold_in(key, 3), (MIX_WIDTH,), jnp.float32, 0.2, 0.6)[None, :]
    slow_value_rows = jnp.log(channel / SEQ) + 0.5
    fast_value = jnp.log(channel) - 2.6
    displacement_anchor = jnp.where(slow, slow_value_rows, fast_value) + shift + noise
    specialist_places = jax.random.randint(jax.random.fold_in(key, 4), (2,), 0, SEQ)
    contiguous_span_length = jnp.any(capacity_locations[:, None] == specialist_places[None, :], axis=1)[:, None]
    return jnp.where(contiguous_span_length, 1.5, displacement_anchor).astype(jnp.bfloat16)


def draw_rate_in(key, part):
    slow = slow_channel_index(key)
    noise = jnp.clip(jax.random.normal(jax.random.fold_in(key, 5), (SEQ, MIX_WIDTH), jnp.float32), -3.0, 3.0)
    slow_value_rows = jnp.log(jnp.float32(19.2) / SEQ) + 0.7 * noise
    return jnp.where(slow, slow_value_rows, noise).astype(jnp.bfloat16)


def block_scale(rng, shape, shards, least, largest):
    def one(position, shards_of):
        steps = jax.random.uniform(jax.random.fold_in(jax.random.fold_in(rng, 6), position), (shards_of,), jnp.float32, least / len(shards), largest / len(shards))
        return jnp.repeat(jnp.exp(steps), shape[position] // shards_of).reshape((-1,) + (1,) * (len(shape) - position - 1))

    level = one(*shards[0])
    for cut in shards[1:]:
        level = level * one(*cut)
    return level


def shared_out(key, own, number, rows, number_of, top, bound, slope):
    order = jax.random.permutation(key, number_of)
    heavy_load, ordinary = load_shares(number_of, rows * top, bound, slope, True), load_shares(number_of, rows * top, bound, slope, False)
    places = jnp.arange(number_of)

    def named(sizes, offset_by):
        used = int((sizes > 0).sum())
        fixed = max(1, used // 4)
        passed = fixed + (places - fixed + offset_by * (used - fixed)) % max(1, number_of - fixed)
        return jnp.zeros((number_of,), jnp.int32).at[order[jnp.where(places < fixed, places, passed)]].set(jnp.asarray(sizes, jnp.int32))

    sizes = jnp.where(number % 4 == 0, named(heavy_load, number // 4), named(ordinary, number - number // 4 - 1))
    mixed = jax.random.permutation(jax.random.fold_in(own, 3), number_of)
    source_of, receiver = mixed[0:number_of // 2 * 2:2], mixed[1:number_of // 2 * 2:2]
    room = jnp.minimum(sizes[source_of] - 1, bound - sizes[receiver]) // 2
    room = jnp.where((source_of == order[0]) | (receiver == order[0]) | (sizes[receiver] == 0), 0, jnp.maximum(room, 0))
    passed = jax.random.randint(jax.random.fold_in(own, 4), (number_of // 2,), 0, 1 << 20) % (room + 1)
    sizes = sizes.at[source_of].add(-passed).at[receiver].add(passed)
    members = jnp.searchsorted(jnp.cumsum(sizes), jnp.arange(rows * top), side="right").astype(jnp.int32)
    table = members.reshape(top, rows).T
    table = table[jax.random.permutation(jax.random.fold_in(own, 1), rows)]
    offset_by = jax.random.randint(jax.random.fold_in(own, 2), (rows, 1), 0, top)
    return jnp.take_along_axis(table, (jnp.arange(top)[None, :] + offset_by) % top, axis=1)


def load_shares(amount, total, bound, skew, full):
    loads = [(1 << 20) // math.isqrt(standing ** skew) + 1 for standing in range(1, amount + 1)]
    largest = bound if full else min(bound, max(-(-total // amount), total * loads[0] // sum(loads)))
    least = 1 if total - largest >= amount - 1 else 0
    holding, surplus = [largest] + [least] * (amount - 1), total - largest - least * (amount - 1)
    while surplus > 0:
        movable = [i for i in range(1, amount) if holding[i] < largest] or [i for i in range(1, amount) if holding[i] < bound]
        pool, remaining = sum([loads[i] for i in movable]), surplus
        for i in movable:
            more = min(bound - holding[i], max(1, remaining * loads[i] // pool), surplus)
            holding[i] = holding[i] + more
            surplus = surplus - more
    return np.array(holding)


def scatter_about(own_key, dims, width, reach, pieces=(), held_as=jnp.bfloat16):
    factor_of = block_scale(own_key, dims, pieces, -0.22, 0.18) if pieces else 1.0
    entries = jax.random.normal(own_key, dims, jnp.float32) * width * factor_of
    return jnp.minimum(jnp.maximum(entries, -reach), reach).astype(held_as)


def setup_inputs(seed: int = 0) -> dict:
    arg_keys = jax.random.split(jax.random.key(seed), 19)
    receptance = scatter_about(arg_keys[0], (SEQ, MIX_WIDTH), 1.0, 6.0, ((0, 16), (1, 16)))
    key_in = scatter_about(arg_keys[1], (SEQ, MIX_WIDTH), 1.0, 6.0, ((0, 16), (1, 16)))
    payload_vectors = scatter_about(arg_keys[2], (SEQ, MIX_WIDTH), 1.0, 6.0, ((0, 16), (1, 16)))
    decay_in = draw_decay_in(jax.random.fold_in(arg_keys[18], 71), 0)
    rate_in = draw_rate_in(jax.random.fold_in(arg_keys[18], 71), 0)
    gate_in = scatter_about(arg_keys[5], (SEQ, MIX_WIDTH), 1.0, 6.0, ((0, 16), (1, 16)))
    norm_gain = jnp.clip(1.0 + 0.18 * jax.random.normal(arg_keys[6], (MIX_WIDTH,), jnp.float32), 0.1, 1.9)
    out_weight = scatter_about(arg_keys[7], (MIX_WIDTH, D), MIX_WIDTH ** -0.5, 0.1875, ((0, 16),))
    moe_in = scatter_about(arg_keys[8], (MOE_ALL, D), 1.0, 6.0, ((0, 256),))
    moe_gain = jnp.clip(1.0 + 0.18 * jax.random.normal(arg_keys[9], (D,), jnp.float32), 0.1, 1.9)
    routes_keys = jax.random.split(jax.random.fold_in(arg_keys[10], 1), MOE_ALL // MOE_TOKENS)
    routes_turns = jax.random.permutation(jax.random.fold_in(arg_keys[10], 3), MOE_ALL // MOE_TOKENS)
    routes = jax.vmap(lambda own, number: shared_out(jax.random.fold_in(arg_keys[10], 2), own, number, MOE_TOKENS, EXPERTS, TOP_K, SLOTS, 1))(routes_keys, routes_turns).reshape((MOE_ALL, TOP_K))
    route_weights = jnp.clip(0.2 + 0.8 * jax.random.uniform(arg_keys[11], (MOE_ALL, TOP_K), jnp.float32) ** block_scale(arg_keys[11], (MOE_ALL, TOP_K), ((0, 256),), -0.2, 0.2), 0.2, 1.0)
    expert_gate = scatter_about(arg_keys[12], (EXPERTS, D, EXPERT_WIDTH), D ** -0.5, 0.125, ((0, 16), (2, 16)))
    expert_up = scatter_about(arg_keys[13], (EXPERTS, D, EXPERT_WIDTH), D ** -0.5, 0.125, ((0, 16), (2, 16)))
    expert_down = scatter_about(arg_keys[14], (EXPERTS, D, EXPERT_WIDTH), EXPERT_WIDTH ** -0.5, 0.25, ((0, 16), (2, 16)))
    shared_gate = scatter_about(arg_keys[15], (D, SHARED_WIDTH), D ** -0.5, 0.125)
    shared_up = scatter_about(arg_keys[16], (D, SHARED_WIDTH), D ** -0.5, 0.125)
    shared_down = scatter_about(arg_keys[17], (SHARED_WIDTH, D), SHARED_WIDTH ** -0.5, 0.25)
    return {"receptance": receptance, "key_in": key_in, "payload_vectors": payload_vectors, "decay_in": decay_in, "rate_in": rate_in, "gate_in": gate_in, "norm_gain": norm_gain, "out_weight": out_weight, "moe_in": moe_in, "moe_gain": moe_gain, "routes": routes, "route_weights": route_weights, "expert_gate": expert_gate, "expert_up": expert_up, "expert_down": expert_down, "shared_gate": shared_gate, "shared_up": shared_up, "shared_down": shared_down}


def mult(form, left, right):
    return jnp.einsum(form, left, right, precision=lax.Precision.HIGHEST)

def block_maps(receive, keys, values, log_decay, alpha, beta):
    length = receive.shape[-2]
    cumul = jnp.cumsum(log_decay, axis=-2)
    before = cumul - log_decay
    ending = cumul[..., -1:, :]
    query_dec = receive * jnp.exp(cumul)
    alpha_dec = alpha * jnp.exp(before)
    key_grow = keys * jnp.exp(-cumul)
    beta_grow = beta * jnp.exp(-cumul)
    row_index = jnp.arange(length, dtype=jnp.int32)[:, None]
    col_index = jnp.arange(length, dtype=jnp.int32)[None, :]
    strict = col_index < row_index
    inclusive_cumsum = col_index <= row_index
    couple = jnp.where(strict, mult('...tc,...sc->...ts', alpha_dec, beta_grow), 0.0)
    insert_term = jnp.where(strict, mult('...tc,...sc->...ts', alpha_dec, key_grow), 0.0)
    inverse = jnp.eye(length, dtype=jnp.float32) + couple
    power = couple
    for section in range(length.bit_length() - 2):
        power = mult('...ij,...jk->...ik', power, power)
        inverse = inverse + mult('...ij,...jk->...ik', inverse, power)
    q_rows = mult('...ts,...sc->...tc', inverse, alpha_dec)
    z_rows = mult('...ts,...sv->...tv', inverse, mult('...ts,...sv->...tv', insert_term, values))
    read_beta = jnp.where(inclusive_cumsum, mult('...tc,...sc->...ts', query_dec, beta_grow), 0.0)
    read_key = jnp.where(inclusive_cumsum, mult('...tc,...sc->...ts', query_dec, key_grow), 0.0)
    query_bar = query_dec + mult('...ts,...sc->...tc', read_beta, q_rows)
    local_out = mult('...ts,...sv->...tv', read_beta, z_rows) + mult('...ts,...sv->...tv', read_key, values)
    beta_end = beta * jnp.exp(ending - cumul)
    key_end = keys * jnp.exp(ending - cumul)
    eye = jnp.eye(keys.shape[-1], dtype=jnp.float32)
    carry_map = mult('...tc,...td->...cd', q_rows, beta_end) + jnp.exp(ending)[..., 0, :, None] * eye
    source_map = mult('...tv,...tk->...vk', z_rows, beta_end) + mult('...tv,...tk->...vk', values, key_end)
    return (query_bar, local_out, carry_map, source_map)

def mixer(receptance, key_in, payload_vectors, decay_in, rate_in, gate_in, norm_gain, out_weight):
    length = receptance.shape[0]

    def split_heads(array):
        return array.reshape(length // BLOCK, BLOCK, HEADS, HEAD_DIM).transpose(2, 0, 1, 3)
    keys = split_heads(key_in.astype(jnp.float32))
    unit = keys * lax.rsqrt(lax.optimization_barrier(jnp.sum(keys * keys, -1, keepdims=True)) + 1e-06)
    rate = split_heads(jax.nn.sigmoid(rate_in.astype(jnp.float32)))
    log_decay = split_heads(-jnp.exp(-jax.nn.softplus(-decay_in.astype(jnp.float32)) - 0.5))
    queries = split_heads(receptance.astype(jnp.float32))
    values = split_heads(payload_vectors.astype(jnp.float32))

    def one_head(operands):
        query_h, key_h, value_h, decay_h, alpha_h, beta_h = operands
        query_bar, local_out, carry_map, source_map = block_maps(query_h, key_h, value_h, decay_h, alpha_h, beta_h)

        def advance(state, blocks):
            bar_b, local_b, carry_b, source_b = blocks
            output = mult('tk,vk->tv', bar_b, state) + local_b
            return (mult('ij,jk->ik', state, carry_b) + source_b, output)
        start_state = jnp.zeros((HEAD_DIM, HEAD_DIM), jnp.float32)
        final, outputs = lax.scan(advance, start_state, (query_bar, local_out, carry_map, source_map))
        return outputs
    recur = lax.map(one_head, (queries, keys, values, log_decay, -unit, unit * rate))
    recur = recur.transpose(1, 2, 0, 3).reshape(length, HEADS, HEAD_DIM)
    centered = recur - lax.optimization_barrier(jnp.mean(recur, -1, keepdims=True))
    rescaled_input = centered * lax.rsqrt(lax.optimization_barrier(jnp.mean(centered * centered, -1, keepdims=True)) + 0.00064)
    gated = rescaled_input.reshape(length, MIX_WIDTH) * norm_gain * jax.nn.sigmoid(gate_in.astype(jnp.float32))
    mixer_rows = gated.astype(jnp.bfloat16)
    return jnp.dot(mixer_rows, out_weight, preferred_element_type=jnp.float32).astype(jnp.bfloat16)

def experts(moe_in, moe_gain, routes, route_weights, expert_gate, expert_up, expert_down, shared_gate, shared_up, shared_down):
    tile_rows = 128
    values = moe_in.astype(jnp.float32)
    centered = values - lax.optimization_barrier(jnp.mean(values, -1, keepdims=True))
    rescaled_input = (centered * lax.rsqrt(lax.optimization_barrier(jnp.mean(centered * centered, -1, keepdims=True)) + 1e-05) * moe_gain).astype(jnp.bfloat16)
    shared_gate_out = jnp.dot(rescaled_input, shared_gate, preferred_element_type=jnp.float32)
    shared_up_out = jnp.dot(rescaled_input, shared_up, preferred_element_type=jnp.float32)
    shared_hidden = (jax.nn.silu(shared_gate_out) * shared_up_out).astype(jnp.bfloat16)
    shared_term = jnp.dot(shared_hidden, shared_down, preferred_element_type=jnp.float32)
    share = 2.5 * route_weights / lax.optimization_barrier(jnp.sum(route_weights, -1, keepdims=True))
    tokens = rescaled_input.shape[0]
    pairs = tokens * TOP_K
    flat_expert = routes.reshape(-1).astype(jnp.int32)
    flat_token = jnp.repeat(jnp.arange(tokens, dtype=jnp.int32), TOP_K)
    flat_share = share.reshape(-1)
    order = jnp.argsort(flat_expert, stable=True).astype(jnp.int32)
    sorted_expert = flat_expert[order]
    counts = lax.optimization_barrier(jnp.sum((flat_expert[:, None] == jnp.arange(EXPERTS, dtype=jnp.int32)[None, :]).astype(jnp.int32), 0)).astype(jnp.int32)
    padded = ((counts + tile_rows - 1) // tile_rows * tile_rows).astype(jnp.int32)
    pad_end = jnp.cumsum(padded).astype(jnp.int32)
    pad_start = (pad_end - padded).astype(jnp.int32)
    first = (jnp.cumsum(counts) - counts).astype(jnp.int32)
    dest = (pad_start[sorted_expert] + jnp.arange(pairs, dtype=jnp.int32) - first[sorted_expert]).astype(jnp.int32)
    capacity = (pairs + tile_rows - 1) // tile_rows * tile_rows + EXPERTS * tile_rows
    blocks = capacity // tile_rows
    slot_token = jnp.full((capacity,), tokens, jnp.int32).at[dest].set(flat_token[order])
    slot_share = jnp.zeros((capacity,), jnp.float32).at[dest].set(flat_share[order])
    group_starts = jnp.arange(blocks, dtype=jnp.int32) * tile_rows
    block_expert = jnp.minimum(jnp.searchsorted(pad_end, group_starts, side='right').astype(jnp.int32), EXPERTS - 1).astype(jnp.int32)
    rows_padded = jnp.concatenate([rescaled_input, jnp.zeros((1, rescaled_input.shape[1]), jnp.bfloat16)], axis=0)

    def add_block(total, operands):
        token_ids, weights, expert = operands
        rows = rows_padded[token_ids]
        gate = jnp.dot(rows, expert_gate[expert], preferred_element_type=jnp.float32)
        upper = jnp.dot(rows, expert_up[expert], preferred_element_type=jnp.float32)
        hidden = (jax.nn.silu(gate) * upper).astype(jnp.bfloat16)
        result = jnp.dot(hidden, expert_down[expert].T, preferred_element_type=jnp.float32).astype(jnp.bfloat16)
        return (total.at[token_ids].add(result.astype(jnp.float32) * weights[:, None]), None)
    start_total = jnp.zeros((tokens + 1, rescaled_input.shape[1]), jnp.float32)
    total, unused = lax.scan(add_block, start_total, (slot_token.reshape(blocks, tile_rows), slot_share.reshape(blocks, tile_rows), block_expert))
    return (shared_term + total[:tokens]).astype(jnp.bfloat16)

def reference(receptance, key_in, payload_vectors, decay_in, rate_in, gate_in, norm_gain, out_weight, moe_in, moe_gain, routes, route_weights, expert_gate, expert_up, expert_down, shared_gate, shared_up, shared_down):
    mixed = mixer(receptance, key_in, payload_vectors, decay_in, rate_in, gate_in, norm_gain, out_weight)
    moe_out = experts(moe_in, moe_gain, routes, route_weights, expert_gate, expert_up, expert_down, shared_gate, shared_up, shared_down)
    return (mixed, moe_out)
```

```python
import jax
import jax.numpy as jnp
from jax import lax
from jax.experimental import pallas as pl
from jax.experimental.pallas import tpu as pltpu
from jax.sharding import Mesh
from jax.sharding import PartitionSpec as P

HEAD_DIM = 64
CHUNK = 128
GROUP = 4
SLOTS = 12
EP = ("ep_0", "ep_1")
EP_TP = ("ep_0", "ep_1", "tp")
BF = jnp.bfloat16
F32 = jnp.float32
VMEM_LIMIT = 56 * 1024 * 1024


def iota(shape, axis):
    return lax.broadcasted_iota(jnp.int32, shape, axis)


def mm(left, right):
    return jnp.dot(left.astype(BF), right.astype(BF), preferred_element_type=F32)


def mm3(left, right):
    left_high, right_high = left.astype(BF), right.astype(BF)
    left_low, right_low = left - left_high.astype(F32), right - right_high.astype(F32)
    return mm(left_high, right_high) + (mm(left_high, right_low) + mm(left_low, right_high))


def dot_dims(left, right, dims):
    return lax.dot_general(left, right, (dims, ((), ())), preferred_element_type=F32)


def scan_kernel(key_ref, recept_ref, value_ref, decay_ref, rate_ref, reads_ref, total_ref):
    dim, length = key_ref.shape
    n = CHUNK
    row, col = iota((n, n), 0), iota((n, n), 1)
    strict, inclusive = col < row, col <= row
    eye = (row == col).astype(F32)
    near = (row >> 4) == (col >> 4)
    bands = [
        ((row >> (k + 1)) == (col >> (k + 1))) & ((row >> k) != (col >> k)) for k in (4, 5, 6)
    ]
    left_half = col < dim
    upper = (row <= col).astype(BF)
    upper3 = jnp.concatenate([upper, upper, upper], axis=0)
    zero_dim = jnp.zeros((dim, n), F32)
    zero_pair = jnp.zeros((dim, 2 * n), BF)
    left_dim = iota((dim, n), 1) < dim

    def one_group(g, state):
        stage = []
        for j in range(GROUP):
            at = pl.ds(pl.multiple_of((g * GROUP + j) * n, n), n)
            keys = key_ref[:, at].astype(F32)
            recept = recept_ref[:, at].astype(F32)
            values = value_ref[:, at].astype(F32)
            unit = keys * lax.rsqrt(jnp.sum(keys * keys, axis=0, keepdims=True) + 1e-6)
            beta = unit * jax.nn.sigmoid(rate_ref[:, at].astype(F32))
            log_decay = jax.nn.sigmoid(decay_ref[:, at].astype(F32)) * (-0.6065306597126334)
            high = log_decay.astype(BF)
            rest = log_decay - high.astype(F32)
            mid = rest.astype(BF)
            low = (rest - mid.astype(F32)).astype(BF)
            cumul = jnp.dot(
                jnp.concatenate([high, mid, low], axis=1), upper3, preferred_element_type=F32
            )
            ending = cumul[:, n - 1 : n]
            grow = jnp.exp(-cumul)
            to_end = jnp.exp(ending - cumul)
            alpha_dec = -unit * jnp.exp(cumul - log_decay)
            query_dec = recept * jnp.exp(cumul)
            pair = jnp.concatenate([(beta * grow).astype(BF), (keys * grow).astype(BF)], axis=1)
            rows = jnp.concatenate([alpha_dec, query_dec], axis=0).T
            stage.append(
                dict(
                    rows=rows,
                    pair=jnp.concatenate(
                        [
                            jnp.concatenate([pair, zero_pair], axis=1),
                            jnp.concatenate([zero_pair, pair], axis=1),
                        ],
                        axis=0,
                    ),
                    value_rows=jnp.concatenate([zero_dim, values], axis=0).T,
                    beta_end=beta * to_end,
                    key_end=keys * to_end,
                    decay_all=jnp.exp(ending),
                )
            )
        for s in stage:
            scores = mm(s["rows"], s["pair"])
            s["couple"] = jnp.where(strict, scores[:, :n], 0.0)
            s["insert"] = jnp.where(strict, scores[:, n : 2 * n], 0.0)
            s["read_beta"] = jnp.where(inclusive, scores[:, 2 * n : 3 * n], 0.0)
            s["read_key"] = jnp.where(inclusive, scores[:, 3 * n :], 0.0)
        for s in stage:
            block = jnp.where(near, s["couple"], 0.0)
            s["inv"] = eye + block
            s["power"] = mm(block, block)
        for step in range(2):
            for s in stage:
                both = mm(jnp.concatenate([s["inv"], s["power"]], axis=0), s["power"])
                s["inv"] = s["inv"] + both[:n]
                s["power"] = both[n:]
        for s in stage:
            s["inv"] = s["inv"] + mm(s["inv"], s["power"])
        for band in bands:
            for s in stage:
                s["side"] = mm(jnp.where(band, s["couple"], 0.0), s["inv"])
            for s in stage:
                s["inv"] = s["inv"] + mm(s["inv"], s["side"])
        for s in stage:
            s["through"] = mm(jnp.concatenate([s["read_beta"], s["beta_end"]], axis=0), s["inv"])
        for s in stage:
            direct = jnp.concatenate([s["read_key"], s["key_end"]], axis=0)
            s["direct"] = mm(s["through"], s["insert"]) + direct
        for s in stage:
            sources = jnp.concatenate(
                [jnp.where(left_half, s["rows"], 0.0), s["value_rows"]], axis=0
            )
            maps = mm(jnp.concatenate([s["through"], s["direct"]], axis=1), sources)
            query = jnp.where(left_half, pltpu.roll(s["rows"], dim, 1), 0.0)
            s["reads"] = maps[:n] + query
            s["moves"] = maps[n:]
        for j, s in enumerate(stage):
            at = pl.ds(pl.multiple_of((g * GROUP + j) * n, n), n)
            left = jnp.concatenate([s["reads"], s["moves"]], axis=0)[:, :dim]
            met = mm(left, state)
            out = met[:n] + jnp.where(left_half, 0.0, s["reads"])
            reads_ref[:, at] = out.T
            state = s["decay_all"] * state + met[n:] + jnp.where(left_dim, 0.0, s["moves"])
        return state

    start = (iota((dim, n), 0) == iota((dim, n), 1)).astype(F32)
    total_ref[...] = lax.fori_loop(0, length // (n * GROUP), one_group, start)


def gate_kernel(here_ref, totals_ref, reads_ref, gate_ref, gain_ref, out_ref):
    dim = gate_ref.shape[0]
    right = iota((dim, 2 * dim), 1) >= dim

    def pass_device(d, entry):
        total = totals_ref[d]
        moved = mm3(total[:, :dim], entry)
        return jnp.where(right, moved + total, 0.0)

    entry = lax.fori_loop(0, here_ref[0], pass_device, jnp.zeros((dim, 2 * dim), F32))
    entry = jnp.concatenate([entry, jnp.zeros_like(entry)], axis=0).T[dim:, :dim]
    gain = jnp.broadcast_to(gain_ref[...], (dim, dim))
    same = iota((dim, dim), 0) == iota((dim, dim), 1)
    gain = jnp.sum(jnp.where(same, gain, 0.0), axis=1, keepdims=True)
    parts = out_ref.shape[0]
    n = out_ref.shape[2]
    step = 4

    for j in range(0, parts, step):
        at = slice(j * n, (j + step) * n)
        recur = mm(entry, reads_ref[:dim, at]) + reads_ref[dim:, at]
        centered = recur - jnp.mean(recur, axis=0, keepdims=True)
        spread = jnp.mean(centered * centered, axis=0, keepdims=True)
        normed = centered * lax.rsqrt(spread + 0.00064)
        gated = normed * gain * jax.nn.sigmoid(gate_ref[:, at].astype(F32))
        for k in range(step):
            out_ref[j + k] = gated[:, k * n : (k + 1) * n].astype(BF)


def slot_tables(routes, total, experts):
    tokens = routes.shape[1]
    expert = iota((experts, tokens), 0)
    first, second = routes[0:1] == expert, routes[1:2] == expert
    picked = first | second
    before = (iota((tokens, tokens), 0) < iota((tokens, tokens), 1)).astype(BF)
    rank = mm(picked.astype(F32), before)
    marked = jnp.where(picked, rank + 1.0, 0.0)

    def places(shape):
        r = iota(shape, 0)
        group = (r * 2731) >> 16
        q = r - group * 24
        odd = ((q >= 8) & (q < 16)) | (q >= 20)
        base = jnp.where(q < 8, 0, jnp.where(q < 16, 8, jnp.where(q < 20, 8, 12)))
        return group * 2 + odd.astype(jnp.int32), q - base

    owner, unused = places((total, experts))
    spread = (owner == iota((total, experts), 1)).astype(F32)
    unused, place = places((total, tokens))
    filled = mm(spread, marked) == (place + 1).astype(F32)
    return first, second, spread, filled


def dispatch_kernel(moe_ref, gain_ref, routes_ref, normed_ref, sent_ref):
    values = moe_ref[...].astype(F32)
    centered = values - jnp.mean(values, axis=1, keepdims=True)
    spread = jnp.mean(centered * centered, axis=1, keepdims=True)
    normed = (centered * lax.rsqrt(spread + 1e-05) * gain_ref[...]).astype(BF)
    normed_ref[...] = normed
    total = sent_ref.shape[0]
    filled = slot_tables(routes_ref[...], total, total // SLOTS)[3]
    sent_ref[...] = mm(filled.astype(F32), normed).astype(BF)


def expert_kernel(rows_ref, weights_ref, out_ref, sum_ref):
    e, half = pl.program_id(0), pl.program_id(1)
    groups, slots, width = rows_ref.shape
    rows = groups * 8
    hidden = weights_ref.shape[0] * weights_ref.shape[3]

    @pl.when((e == 0) & (half == 0))
    def _():
        sum_ref[...] = jnp.zeros_like(sum_ref)

    def go(which):
        own = rows_ref[:, 8 * which : 8 * which + 8].reshape(rows, width)
        shared = rows_ref[:, 16:24].reshape(rows, width)
        given = jnp.concatenate([own, shared], axis=0)
        gate = dot_dims(given, weights_ref[:, 0, 0].reshape(hidden, width), ((1,), (1,)))
        upper = dot_dims(given, weights_ref[:, 1, 0].reshape(hidden, width), ((1,), (1,)))
        act = gate * jax.nn.sigmoid(gate) * upper
        r = iota(act.shape, 0)
        mine = (r < rows) | (((r & 7) >= 4) == (which == 1))
        act = jnp.where(mine, act, 0.0).astype(BF)
        down = weights_ref[:, 2, 0].reshape(hidden, width)
        sum_ref[which * rows : (which + 1) * rows] += dot_dims(act[:rows], down, ((1,), (0,)))
        sum_ref[2 * rows :] += dot_dims(act[rows:], down, ((1,), (0,)))

    @pl.when(e == 0)
    def _():
        go(0)

    @pl.when(e == 1)
    def _():
        go(1)

    @pl.when((e == 1) & (half == 1))
    def _():
        for k in range(3):
            part = sum_ref[k * rows : (k + 1) * rows].reshape(groups, 8, width)
            out_ref[:, 8 * k : 8 * k + 8] = part.astype(BF)


def combine_kernel(routes_ref, weights_ref, results_ref, shared_ref, out_ref):
    total = results_ref.shape[0]
    first, second, spread, filled = slot_tables(routes_ref[...], total, total // SLOTS)
    weights = weights_ref[...]
    share = 2.5 * weights / jnp.sum(weights, axis=0, keepdims=True)
    chosen = jnp.where(first, share[0:1], 0.0) + jnp.where(second, share[1:2], 0.0)
    high = chosen.astype(BF).astype(F32)
    results = results_ref[...]
    out = shared_ref[...]
    for part in (high, chosen - high):
        taken = jnp.where(filled, mm(spread, part), 0.0)
        out = out + mm(taken.T, results)
    out_ref[...] = out.astype(BF)


def project_kernel(rows_ref, weight_ref, out_ref):
    out_ref[...] = dot_dims(rows_ref[...], weight_ref[...], ((0,), (0,))).astype(BF)


def call(kernel, out_shape, **options):
    return pl.pallas_call(
        kernel,
        out_shape=out_shape,
        name=kernel.__name__,
        compiler_params=pltpu.CompilerParams(vmem_limit_bytes=VMEM_LIMIT),
        **options,
    )


def shape(dims, dtype):
    return jax.ShapeDtypeStruct(dims, dtype)


def shards(
    receptance,
    key_in,
    payload_vectors,
    decay_in,
    rate_in,
    gate_in,
    norm_gain,
    out_weight,
    moe_in,
    moe_gain,
    routes,
    route_weights,
    expert_gate,
    expert_up,
    expert_down,
    shared_gate,
    shared_up,
    shared_down,
):
    groups, peers = lax.axis_size(EP), lax.axis_size("tp")
    here = lax.axis_index(EP)
    length, dim = key_in.shape
    tokens, width = moe_in.shape

    local_weights = jnp.stack([w.transpose(0, 2, 1) for w in (expert_gate, expert_up, expert_down)])
    all_weights = lax.all_gather(local_weights, "tp")
    out_weight, unused = lax.optimization_barrier((out_weight, local_weights))
    projection = lax.all_gather(out_weight, "tp", axis=0, tiled=True)

    slots = expert_gate.shape[0] * SLOTS
    normed, sent = call(
        dispatch_kernel,
        (shape((tokens, width), BF), shape((groups * slots, width), BF)),
    )(moe_in, moe_gain.reshape(1, width), routes.T)
    arrived = lax.all_to_all(
        sent.reshape(groups, slots, width), EP, split_axis=0, concat_axis=0, tiled=True
    )

    reads, total = call(
        scan_kernel, (shape((2 * dim, length), F32), shape((dim, 2 * dim), F32))
    )(key_in.T, receptance.T, payload_vectors.T, decay_in.T, rate_in.T)
    totals = lax.all_to_all(
        jnp.broadcast_to(total, (groups, dim, 2 * dim)),
        EP,
        split_axis=0,
        concat_axis=0,
        tiled=True,
    )
    smem = pl.BlockSpec(memory_space=pltpu.SMEM)
    vmem = pl.BlockSpec(memory_space=pltpu.VMEM)
    rows = call(
        gate_kernel,
        shape((peers, dim, length // peers), BF),
        in_specs=[smem] + [vmem] * 4,
    )(here.astype(jnp.int32).reshape(1), totals, reads, gate_in.T, norm_gain.reshape(1, dim))
    token_rows = lax.all_to_all(rows, "tp", split_axis=0, concat_axis=0, tiled=True)

    gate = jnp.dot(normed, shared_gate, preferred_element_type=F32)
    upper = jnp.dot(normed, shared_up, preferred_element_type=F32)
    hidden = (jax.nn.silu(gate) * upper).astype(BF)
    shared_term = jnp.dot(hidden, shared_down, preferred_element_type=F32)

    part = peers // 2
    units = expert_gate.shape[2]
    results = call(
        expert_kernel,
        shape((groups, slots, width), BF),
        grid=(2, 2),
        in_specs=[
            pl.BlockSpec((groups, slots, width), lambda e, h: (0, 0, 0)),
            pl.BlockSpec((part, 3, 1, units, width), lambda e, h: (h, 0, e, 0, 0)),
        ],
        out_specs=pl.BlockSpec((groups, slots, width), lambda e, h: (0, 0, 0)),
        scratch_shapes=[pltpu.VMEM((groups * slots, width), F32)],
    )(arrived, all_weights)
    returned = lax.all_to_all(results, EP, split_axis=0, concat_axis=0, tiled=True)
    moe_out = call(combine_kernel, shape((tokens, width), BF))(
        routes.T, route_weights.T, returned.reshape(groups * slots, width), shared_term
    )

    columns = width // 8
    mixed = call(
        project_kernel,
        shape((tokens, width), BF),
        grid=(width // columns,),
        in_specs=[
            pl.BlockSpec((peers * dim, tokens), lambda i: (0, 0)),
            pl.BlockSpec((peers * dim, columns), lambda i: (0, i)),
        ],
        out_specs=pl.BlockSpec((tokens, columns), lambda i: (0, i)),
    )(token_rows.reshape(peers * dim, tokens), projection)
    return (mixed, moe_out)


def solution(mesh):
    torus = Mesh(mesh.devices.reshape(4, 4, mesh.shape["tp"]), ("ep_0", "ep_1", "tp"))
    placed = (
        *(P(EP, "tp"),) * 6,
        P("tp"),
        P("tp", None),
        P(EP_TP, None),
        P(),
        P(EP_TP, None),
        P(EP_TP, None),
        *(P(EP, None, "tp"),) * 3,
        P(),
        P(),
        P(),
    )
    return jax.shard_map(
        shards,
        mesh=torus,
        in_specs=placed,
        out_specs=(P(EP_TP, None), P(EP_TP, None)),
        check_vma=False,
    )
```

```python
import jax
import jax.numpy as jnp
from jax import lax
from jax.experimental import pallas as pl
from jax.experimental.pallas import tpu as pltpu
from jax.sharding import Mesh
from jax.sharding import PartitionSpec as P


CHUNK = 128
GROUP = 4
SLOTS = 12
EP = ("ep_0", "ep_1")
TP = ("z", "core")
EP_TP = EP + TP
BF = jnp.bfloat16
F32 = jnp.float32
VMEM_LIMIT = 56 * 1024 * 1024


def iota(shape, axis):
    return lax.broadcasted_iota(jnp.int32, shape, axis)


def mm(left, right):
    return jnp.dot(left.astype(BF), right.astype(BF), preferred_element_type=F32)


def mm3(left, right):
    left_high, right_high = left.astype(BF), right.astype(BF)
    left_low, right_low = left - left_high.astype(F32), right - right_high.astype(F32)
    return mm(left_high, right_high) + (mm(left_high, right_low) + mm(left_low, right_high))


def dot_dims(left, right, dims):
    return lax.dot_general(left, right, (dims, ((), ())), preferred_element_type=F32)


def scan_kernel(key_ref, recept_ref, value_ref, decay_ref, rate_ref, reads_ref, total_ref):
    dim, length = key_ref.shape
    n = CHUNK
    row, col = iota((n, n), 0), iota((n, n), 1)
    strict, inclusive = col < row, col <= row
    eye = (row == col).astype(F32)
    near = (row >> 4) == (col >> 4)
    bands = [
        ((row >> (k + 1)) == (col >> (k + 1))) & ((row >> k) != (col >> k)) for k in (4, 5, 6)
    ]
    left_half = col < dim
    upper = (row <= col).astype(BF)
    upper3 = jnp.concatenate([upper, upper, upper], axis=0)
    zero_dim = jnp.zeros((dim, n), F32)
    zero_pair = jnp.zeros((dim, 2 * n), BF)
    left_dim = iota((dim, n), 1) < dim

    def one_group(g, state):
        stage = []
        for j in range(GROUP):
            at = pl.ds(pl.multiple_of((g * GROUP + j) * n, n), n)
            keys = key_ref[:, at].astype(F32)
            recept = recept_ref[:, at].astype(F32)
            values = value_ref[:, at].astype(F32)
            unit = keys * lax.rsqrt(jnp.sum(keys * keys, axis=0, keepdims=True) + 1e-6)
            beta = unit * jax.nn.sigmoid(rate_ref[:, at].astype(F32))
            log_decay = jax.nn.sigmoid(decay_ref[:, at].astype(F32)) * (-0.6065306597126334)
            high = log_decay.astype(BF)
            rest = log_decay - high.astype(F32)
            mid = rest.astype(BF)
            low = (rest - mid.astype(F32)).astype(BF)
            cumul = jnp.dot(
                jnp.concatenate([high, mid, low], axis=1), upper3, preferred_element_type=F32
            )
            ending = cumul[:, n - 1 : n]
            grow = jnp.exp(-cumul)
            to_end = jnp.exp(ending - cumul)
            alpha_dec = -unit * jnp.exp(cumul - log_decay)
            query_dec = recept * jnp.exp(cumul)
            pair = jnp.concatenate([(beta * grow).astype(BF), (keys * grow).astype(BF)], axis=1)
            rows = jnp.concatenate([alpha_dec, query_dec], axis=0).T
            stage.append(
                dict(
                    rows=rows,
                    pair=jnp.concatenate(
                        [
                            jnp.concatenate([pair, zero_pair], axis=1),
                            jnp.concatenate([zero_pair, pair], axis=1),
                        ],
                        axis=0,
                    ),
                    value_rows=jnp.concatenate([zero_dim, values], axis=0).T,
                    beta_end=beta * to_end,
                    key_end=keys * to_end,
                    decay_all=jnp.exp(ending),
                )
            )
        for s in stage:
            scores = mm(s["rows"], s["pair"])
            s["couple"] = jnp.where(strict, scores[:, :n], 0.0)
            s["insert"] = jnp.where(strict, scores[:, n : 2 * n], 0.0)
            s["read_beta"] = jnp.where(inclusive, scores[:, 2 * n : 3 * n], 0.0)
            s["read_key"] = jnp.where(inclusive, scores[:, 3 * n :], 0.0)
        for s in stage:
            block = jnp.where(near, s["couple"], 0.0)
            s["inv"] = eye + block
            s["power"] = mm(block, block)
        for _ in range(2):
            for s in stage:
                both = mm(jnp.concatenate([s["inv"], s["power"]], axis=0), s["power"])
                s["inv"] = s["inv"] + both[:n]
                s["power"] = both[n:]
        for s in stage:
            s["inv"] = s["inv"] + mm(s["inv"], s["power"])
        for band in bands:
            for s in stage:
                s["side"] = mm(jnp.where(band, s["couple"], 0.0), s["inv"])
            for s in stage:
                s["inv"] = s["inv"] + mm(s["inv"], s["side"])
        for s in stage:
            s["through"] = mm(jnp.concatenate([s["read_beta"], s["beta_end"]], axis=0), s["inv"])
        for s in stage:
            direct = jnp.concatenate([s["read_key"], s["key_end"]], axis=0)
            s["direct"] = mm(s["through"], s["insert"]) + direct
        for s in stage:
            sources = jnp.concatenate(
                [jnp.where(left_half, s["rows"], 0.0), s["value_rows"]], axis=0
            )
            maps = mm(jnp.concatenate([s["through"], s["direct"]], axis=1), sources)
            query = jnp.where(left_half, pltpu.roll(s["rows"], dim, 1), 0.0)
            s["reads"] = maps[:n] + query
            s["moves"] = maps[n:]
        for j, s in enumerate(stage):
            at = pl.ds(pl.multiple_of((g * GROUP + j) * n, n), n)
            left = jnp.concatenate([s["reads"], s["moves"]], axis=0)[:, :dim]
            met = mm(left, state)
            out = met[:n] + jnp.where(left_half, 0.0, s["reads"])
            reads_ref[:, at] = out.T
            state = s["decay_all"] * state + met[n:] + jnp.where(left_dim, 0.0, s["moves"])
        return state

    start = (iota((dim, n), 0) == iota((dim, n), 1)).astype(F32)
    total_ref[...] = lax.fori_loop(0, length // (n * GROUP), one_group, start)


def gate_kernel(here_ref, totals_ref, reads_ref, gate_ref, gain_ref, out_ref):
    dim = gate_ref.shape[0]
    right = iota((dim, 2 * dim), 1) >= dim

    def pass_device(d, entry):
        total = totals_ref[d]
        moved = mm3(total[:, :dim], entry)
        return jnp.where(right, moved + total, 0.0)

    entry = lax.fori_loop(0, here_ref[0], pass_device, jnp.zeros((dim, 2 * dim), F32))
    entry = jnp.concatenate([entry, jnp.zeros_like(entry)], axis=0).T[dim:, :dim]
    gain = jnp.broadcast_to(gain_ref[...], (dim, dim))
    same = iota((dim, dim), 0) == iota((dim, dim), 1)
    gain = jnp.sum(jnp.where(same, gain, 0.0), axis=1, keepdims=True)
    parts = out_ref.shape[0]
    n = out_ref.shape[2]
    step = 4

    for j in range(0, parts, step):
        at = slice(j * n, (j + step) * n)
        recur = mm(entry, reads_ref[:dim, at]) + reads_ref[dim:, at]
        centered = recur - jnp.mean(recur, axis=0, keepdims=True)
        spread = jnp.mean(centered * centered, axis=0, keepdims=True)
        normed = centered * lax.rsqrt(spread + 0.00064)
        gated = normed * gain * jax.nn.sigmoid(gate_ref[:, at].astype(F32))
        for k in range(step):
            out_ref[j + k] = gated[:, k * n : (k + 1) * n].astype(BF)


def slot_tables(routes, total, experts):
    tokens = routes.shape[1]
    expert = iota((experts, tokens), 0)
    first, second = routes[0:1] == expert, routes[1:2] == expert
    picked = first | second
    before = (iota((tokens, tokens), 0) < iota((tokens, tokens), 1)).astype(BF)
    rank = mm(picked.astype(F32), before)
    marked = jnp.where(picked, rank + 1.0, 0.0)

    def places(shape):
        r = iota(shape, 0)
        group = (r * 2731) >> 16
        q = r - group * 24
        odd = ((q >= 8) & (q < 16)) | (q >= 20)
        base = jnp.where(q < 8, 0, jnp.where(q < 16, 8, jnp.where(q < 20, 8, 12)))
        return group * 2 + odd.astype(jnp.int32), q - base

    owner, unused = places((total, experts))
    spread = (owner == iota((total, experts), 1)).astype(F32)
    unused, place = places((total, tokens))
    filled = mm(spread, marked) == (place + 1).astype(F32)
    return first, second, spread, filled


def dispatch_kernel(moe_ref, gain_ref, routes_ref, normed_ref, sent_ref):
    values = moe_ref[...].astype(F32)
    centered = values - jnp.mean(values, axis=1, keepdims=True)
    spread = jnp.mean(centered * centered, axis=1, keepdims=True)
    normed = (centered * lax.rsqrt(spread + 1e-05) * gain_ref[...]).astype(BF)
    normed_ref[...] = normed
    total = sent_ref.shape[0]
    filled = slot_tables(routes_ref[...], total, total // SLOTS)[3]
    sent_ref[...] = mm(filled.astype(F32), normed).astype(BF)


def regroup_kernel(rows_ref, out_ref):
    rows, width = out_ref.shape[1:]
    for k in range(3):
        out_ref[k] = rows_ref[:, 8 * k : 8 * k + 8].reshape(rows, width)


def expert_kernel(rows_ref, weights_ref, out_ref, gates_ref, down_ref, hidden_ref, sems, more):
    groups, _, width = out_ref.shape
    rows = groups * 8
    parts, _, each, units = gates_ref.shape[1:5]
    n = each * units

    def gates_copy(e, q, w):
        source = weights_ref.at[pl.ds(q * each, each), w, e]
        return pltpu.make_async_copy(source, gates_ref.at[e, q, w], sems.at[e, q, w])

    def down_copy(e):
        return pltpu.make_async_copy(weights_ref.at[:, 2, e], down_ref.at[e], more.at[e])

    for e in range(2):
        for q in range(parts):
            for w in range(2):
                gates_copy(e, q, w).start()
    for e in range(2):
        down_copy(e).start()
    r = iota((2 * rows, n), 0)
    for e in range(2):
        given = jnp.concatenate([rows_ref[e], rows_ref[2]], axis=0)
        mine = (r < rows) | (((r & 7) >= 4) == (e == 1))
        for q in range(parts):
            for w in range(2):
                gates_copy(e, q, w).wait()
            gates = dot_dims(given, gates_ref[e, q].reshape(2 * n, width), ((1,), (1,)))
            gate, upper = gates[:, :n], gates[:, n:]
            act = gate * jax.nn.sigmoid(gate) * upper
            hidden_ref[e, :, q * n : (q + 1) * n] = jnp.where(mine, act, 0.0).astype(BF)
    for e in range(2):
        down_copy(e).wait()
    step = 512
    for k in range(0, width, step):
        at = slice(k, k + step)
        first, second = (
            dot_dims(hidden_ref[e], down_ref[e, :, :, at].reshape(parts * n, step), ((1,), (0,)))
            for e in range(2)
        )
        parts_out = (first[:rows], second[:rows], first[rows:] + second[rows:])
        for j, part in enumerate(parts_out):
            out_ref[:, 8 * j : 8 * j + 8, at] = part.astype(BF).reshape(groups, 8, step)


def table_kernel(routes_ref, weights_ref, out_ref):
    total = out_ref.shape[2]
    first, second, spread, filled = slot_tables(routes_ref[...], total, total // SLOTS)
    weights = weights_ref[...]
    share = 2.5 * weights / jnp.sum(weights, axis=0, keepdims=True)
    chosen = jnp.where(first, share[0:1], 0.0) + jnp.where(second, share[1:2], 0.0)
    high = chosen.astype(BF).astype(F32)
    for k, part in enumerate((high, chosen - high)):
        out_ref[k] = jnp.where(filled, mm(spread, part), 0.0).T.astype(BF)


def combine_kernel(tables_ref, results_ref, shared_ref, out_ref):
    results = results_ref[...]
    out = shared_ref[...] + (mm(tables_ref[0], results) + mm(tables_ref[1], results))
    out_ref[...] = out.astype(BF)


def project_kernel(place_ref, rows_ref, *refs):
    *blocks, out_ref = refs
    y, x, core = place_ref[0], place_ref[1], place_ref[2]
    chips = rows_ref.shape[0]
    rows = [rows_ref[z, c] for c in range(2) for z in range(chips)]
    rows = jnp.concatenate(rows, axis=0).T
    forth = jnp.where(core == 0, 3, 1)
    for down, way, ref in zip((0, 1, 3, 2), (1, 1, 3, 1), blocks):
        for right in range(4):
            at = ((y + forth * down) % 4) * 4 + (x + forth * way * (0, 1, 3, 2)[right]) % 4
            out = dot_dims(rows, ref[right], ((1,), (0,)))
            out_ref[:, pl.ds(pl.multiple_of(at * 128, 128), 128)] = out.astype(BF)


def call(kernel, out_shape, **options):
    return pl.pallas_call(
        kernel,
        out_shape=out_shape,
        compiler_params=pltpu.CompilerParams(vmem_limit_bytes=VMEM_LIMIT),
        **options,
    )


def shape(dims, dtype):
    return jax.ShapeDtypeStruct(dims, dtype)


def swap(array, axes):
    return lax.all_to_all(array, axes, split_axis=0, concat_axis=0, tiled=True)


def other_core(array):
    return lax.ppermute(array, "core", [(0, 1), (1, 0)])


def around(block, axis):
    pairs = [(2 * k, (2 * k + 2) % 8) for k in range(4)]
    pairs += [((2 * k + 3) % 8, 2 * k + 1) for k in range(4)]
    came = lax.ppermute(block, (axis, "core"), pairs)
    more = other_core(came)
    last = lax.ppermute(came, (axis, "core"), pairs)
    return [block, came, more, last]


def projection_blocks(out_weight, here):
    columns = out_weight.shape[1] // lax.axis_size(EP)
    chips = lax.axis_size("z")
    piece = lax.dynamic_slice_in_dim(out_weight, here * columns, columns, axis=1)
    heads = swap(jnp.broadcast_to(piece, (chips, *piece.shape)), "z")
    heads = heads.reshape(-1, columns)
    return heads


def shards(
    receptance,
    key_in,
    payload_vectors,
    decay_in,
    rate_in,
    gate_in,
    norm_gain,
    out_weight,
    moe_in,
    moe_gain,
    routes,
    route_weights,
    expert_gate,
    expert_up,
    expert_down,
    shared_gate,
    shared_up,
    shared_down,
):
    groups, peers = lax.axis_size(EP), lax.axis_size(TP)
    here = lax.axis_index(EP)
    length, dim = key_in.shape
    tokens, width = moe_in.shape

    local_weights = jnp.stack([w.transpose(0, 2, 1) for w in (expert_gate, expert_up, expert_down)])
    all_weights = lax.all_gather(local_weights, TP)

    core = lax.axis_index("core")
    heads = projection_blocks(out_weight, here)
    slots = expert_gate.shape[0] * SLOTS
    normed, sent = call(
        dispatch_kernel,
        (shape((tokens, width), BF), shape((groups * slots, width), BF)),
    )(moe_in, moe_gain.reshape(1, width), routes.T)
    sent, heads = lax.optimization_barrier((sent, heads))
    arrived = swap(sent.reshape(groups, slots, width), EP)
    others = other_core(heads)
    block = jnp.concatenate(
        [jnp.where(core == 0, heads, others), jnp.where(core == 0, others, heads)]
    )
    across = jnp.stack(around(block, "ep_1"))
    projection = around(across, "ep_0")

    key_in, sent = lax.optimization_barrier((key_in, sent))
    reads, total = call(
        scan_kernel, (shape((2 * dim, length), F32), shape((dim, 2 * dim), F32))
    )(key_in.T, receptance.T, payload_vectors.T, decay_in.T, rate_in.T)
    total, arrived = lax.optimization_barrier((total, arrived))
    totals = swap(jnp.broadcast_to(total, (groups, dim, 2 * dim)), EP)
    smem = pl.BlockSpec(memory_space=pltpu.SMEM)
    vmem = pl.BlockSpec(memory_space=pltpu.VMEM)
    rows = call(
        gate_kernel,
        shape((peers, dim, length // peers), BF),
        in_specs=[smem] + [vmem] * 4,
    )(here.astype(jnp.int32).reshape(1), totals, reads, gate_in.T, norm_gain.reshape(1, dim))
    token_rows = swap(rows, TP)

    gate = jnp.dot(normed, shared_gate, preferred_element_type=F32)
    upper = jnp.dot(normed, shared_up, preferred_element_type=F32)
    hidden = (jax.nn.silu(gate) * upper).astype(BF)
    shared_term = jnp.dot(hidden, shared_down, preferred_element_type=F32)

    units = expert_gate.shape[2]
    each = 4
    given = call(regroup_kernel, shape((3, groups * 8, width), BF))(arrived)
    tables = call(table_kernel, shape((2, tokens, groups * slots), BF))(routes.T, route_weights.T)
    results = call(
        expert_kernel,
        shape((groups, slots, width), BF),
        in_specs=[vmem, pl.BlockSpec(memory_space=pl.ANY)],
        scratch_shapes=[
            pltpu.VMEM((2, peers // each, 2, each, units, width), BF),
            pltpu.VMEM((2, peers, units, width), BF),
            pltpu.VMEM((2, groups * 16, peers * units), BF),
            pltpu.SemaphoreType.DMA((2, peers // each, 2)),
            pltpu.SemaphoreType.DMA((2,)),
        ],
    )(given, all_weights)
    results, token_rows = lax.optimization_barrier((results, token_rows))
    returned = swap(results, EP)
    moe_out = call(combine_kernel, shape((tokens, width), BF))(
        tables, returned.reshape(groups * slots, width), shared_term
    )

    place = jnp.stack([lax.axis_index(axis) for axis in EP] + [core]).astype(jnp.int32)
    mixed = call(
        project_kernel,
        shape((tokens, width), BF),
        in_specs=[smem] + [vmem] * (1 + len(projection)),
    )(place, token_rows.reshape(peers // 2, 2, dim, tokens), *projection)
    return (mixed, moe_out)


def solution(mesh):
    torus = Mesh(mesh.devices.reshape(4, 4, mesh.shape["tp"] // 2, 2), EP_TP)
    placed = (
        *(P(EP, TP),) * 6,
        P(TP),
        P(TP, None),
        P(EP_TP, None),
        P(),
        P(EP_TP, None),
        P(EP_TP, None),
        *(P(EP, None, TP),) * 3,
        P(),
        P(),
        P(),
    )

    return jax.shard_map(
        shards,
        mesh=torus,
        in_specs=placed,
        out_specs=(P(EP_TP, None), P(EP_TP, None)),
        check_vma=False,
    )
```

```python
import jax
import jax.numpy as jnp
from jax import lax
from jax.experimental import pallas as pl
from jax.experimental.pallas import tpu as pltpu
from jax.sharding import Mesh
from jax.sharding import PartitionSpec as P


CHUNK = 128
GROUP = 4
SLOTS = 12
EP = ("ep_0", "ep_1")
TP = ("z", "core")
EP_TP = EP + TP
BF = jnp.bfloat16
F32 = jnp.float32
VMEM_LIMIT = 56 * 1024 * 1024


def iota(shape, axis):
    return lax.broadcasted_iota(jnp.int32, shape, axis)


def mm(left, right):
    return jnp.dot(left.astype(BF), right.astype(BF), preferred_element_type=F32)


def mm3(left, right):
    left_high, right_high = left.astype(BF), right.astype(BF)
    left_low, right_low = left - left_high.astype(F32), right - right_high.astype(F32)
    return mm(left_high, right_high) + (mm(left_high, right_low) + mm(left_low, right_high))


def dot_dims(left, right, dims):
    return lax.dot_general(left, right, (dims, ((), ())), preferred_element_type=F32)


def scan_kernel(key_ref, recept_ref, value_ref, decay_ref, rate_ref, reads_ref, total_ref):
    dim, length = key_ref.shape
    n = CHUNK
    row, col = iota((n, n), 0), iota((n, n), 1)
    strict, inclusive = col < row, col <= row
    eye = (row == col).astype(F32)
    near = (row >> 4) == (col >> 4)
    bands = [
        ((row >> (k + 1)) == (col >> (k + 1))) & ((row >> k) != (col >> k)) for k in (4, 5, 6)
    ]
    left_half = col < dim
    upper = (row <= col).astype(BF)
    upper3 = jnp.concatenate([upper, upper, upper], axis=0)
    zero_dim = jnp.zeros((dim, n), F32)
    zero_pair = jnp.zeros((dim, 2 * n), BF)
    left_dim = iota((dim, n), 1) < dim

    def one_group(g, state):
        stage = []
        for j in range(GROUP):
            at = pl.ds(pl.multiple_of((g * GROUP + j) * n, n), n)
            keys = key_ref[:, at].astype(F32)
            recept = recept_ref[:, at].astype(F32)
            values = value_ref[:, at].astype(F32)
            unit = keys * lax.rsqrt(jnp.sum(keys * keys, axis=0, keepdims=True) + 1e-6)
            beta = unit * jax.nn.sigmoid(rate_ref[:, at].astype(F32))
            log_decay = jax.nn.sigmoid(decay_ref[:, at].astype(F32)) * (-0.6065306597126334)
            high = log_decay.astype(BF)
            rest = log_decay - high.astype(F32)
            mid = rest.astype(BF)
            low = (rest - mid.astype(F32)).astype(BF)
            cumul = jnp.dot(
                jnp.concatenate([high, mid, low], axis=1), upper3, preferred_element_type=F32
            )
            ending = cumul[:, n - 1 : n]
            grow = jnp.exp(-cumul)
            to_end = jnp.exp(ending - cumul)
            alpha_dec = -unit * jnp.exp(cumul - log_decay)
            query_dec = recept * jnp.exp(cumul)
            pair = jnp.concatenate([(beta * grow).astype(BF), (keys * grow).astype(BF)], axis=1)
            rows = jnp.concatenate([alpha_dec, query_dec], axis=0).T
            stage.append(
                dict(
                    rows=rows,
                    pair=jnp.concatenate(
                        [
                            jnp.concatenate([pair, zero_pair], axis=1),
                            jnp.concatenate([zero_pair, pair], axis=1),
                        ],
                        axis=0,
                    ),
                    value_rows=jnp.concatenate([zero_dim, values], axis=0).T,
                    beta_end=beta * to_end,
                    key_end=keys * to_end,
                    decay_all=jnp.exp(ending),
                )
            )
        for s in stage:
            scores = mm(s["rows"], s["pair"])
            s["couple"] = jnp.where(strict, scores[:, :n], 0.0)
            s["insert"] = jnp.where(strict, scores[:, n : 2 * n], 0.0)
            s["read_beta"] = jnp.where(inclusive, scores[:, 2 * n : 3 * n], 0.0)
            s["read_key"] = jnp.where(inclusive, scores[:, 3 * n :], 0.0)
        for s in stage:
            block = jnp.where(near, s["couple"], 0.0)
            s["inv"] = eye + block
            s["power"] = mm(block, block)
        for _ in range(2):
            for s in stage:
                both = mm(jnp.concatenate([s["inv"], s["power"]], axis=0), s["power"])
                s["inv"] = s["inv"] + both[:n]
                s["power"] = both[n:]
        for s in stage:
            s["inv"] = s["inv"] + mm(s["inv"], s["power"])
        for band in bands:
            for s in stage:
                s["side"] = mm(jnp.where(band, s["couple"], 0.0), s["inv"])
            for s in stage:
                s["inv"] = s["inv"] + mm(s["inv"], s["side"])
        for s in stage:
            s["through"] = mm(jnp.concatenate([s["read_beta"], s["beta_end"]], axis=0), s["inv"])
        for s in stage:
            direct = jnp.concatenate([s["read_key"], s["key_end"]], axis=0)
            s["direct"] = mm(s["through"], s["insert"]) + direct
        for s in stage:
            sources = jnp.concatenate(
                [jnp.where(left_half, s["rows"], 0.0), s["value_rows"]], axis=0
            )
            maps = mm(jnp.concatenate([s["through"], s["direct"]], axis=1), sources)
            query = jnp.where(left_half, pltpu.roll(s["rows"], dim, 1), 0.0)
            s["reads"] = maps[:n] + query
            s["moves"] = maps[n:]
        for j, s in enumerate(stage):
            at = pl.ds(pl.multiple_of((g * GROUP + j) * n, n), n)
            left = jnp.concatenate([s["reads"], s["moves"]], axis=0)[:, :dim]
            met = mm(left, state)
            out = met[:n] + jnp.where(left_half, 0.0, s["reads"])
            reads_ref[:, at] = out.T
            state = s["decay_all"] * state + met[n:] + jnp.where(left_dim, 0.0, s["moves"])
        return state

    start = (iota((dim, n), 0) == iota((dim, n), 1)).astype(F32)
    total_ref[...] = lax.fori_loop(0, length // (n * GROUP), one_group, start)


def gate_kernel(here_ref, totals_ref, reads_ref, gate_ref, gain_ref, out_ref):
    dim = gate_ref.shape[0]
    right = iota((dim, 2 * dim), 1) >= dim

    def pass_device(d, entry):
        total = totals_ref[d]
        moved = mm3(total[:, :dim], entry)
        return jnp.where(right, moved + total, 0.0)

    entry = lax.fori_loop(0, here_ref[0], pass_device, jnp.zeros((dim, 2 * dim), F32))
    entry = jnp.concatenate([entry, jnp.zeros_like(entry)], axis=0).T[dim:, :dim]
    gain = jnp.broadcast_to(gain_ref[...], (dim, dim))
    same = iota((dim, dim), 0) == iota((dim, dim), 1)
    gain = jnp.sum(jnp.where(same, gain, 0.0), axis=1, keepdims=True)
    parts = out_ref.shape[0]
    n = out_ref.shape[2]
    step = 4

    for j in range(0, parts, step):
        at = slice(j * n, (j + step) * n)
        recur = mm(entry, reads_ref[:dim, at]) + reads_ref[dim:, at]
        centered = recur - jnp.mean(recur, axis=0, keepdims=True)
        spread = jnp.mean(centered * centered, axis=0, keepdims=True)
        normed = centered * lax.rsqrt(spread + 0.00064)
        gated = normed * gain * jax.nn.sigmoid(gate_ref[:, at].astype(F32))
        for k in range(step):
            out_ref[j + k] = gated[:, k * n : (k + 1) * n].astype(BF)


def slot_tables(routes, total, experts):
    tokens = routes.shape[1]
    expert = iota((experts, tokens), 0)
    first, second = routes[0:1] == expert, routes[1:2] == expert
    picked = first | second
    before = (iota((tokens, tokens), 0) < iota((tokens, tokens), 1)).astype(BF)
    rank = mm(picked.astype(F32), before)
    marked = jnp.where(picked, rank + 1.0, 0.0)

    def places(shape):
        r = iota(shape, 0)
        group = (r * 2731) >> 16
        q = r - group * 24
        odd = ((q >= 8) & (q < 16)) | (q >= 20)
        base = jnp.where(q < 8, 0, jnp.where(q < 16, 8, jnp.where(q < 20, 8, 12)))
        return group * 2 + odd.astype(jnp.int32), q - base

    owner, unused = places((total, experts))
    spread = (owner == iota((total, experts), 1)).astype(F32)
    unused, place = places((total, tokens))
    filled = mm(spread, marked) == (place + 1).astype(F32)
    return first, second, spread, filled


def dispatch_kernel(moe_ref, gain_ref, routes_ref, normed_ref, sent_ref):
    values = moe_ref[...].astype(F32)
    centered = values - jnp.mean(values, axis=1, keepdims=True)
    spread = jnp.mean(centered * centered, axis=1, keepdims=True)
    normed = (centered * lax.rsqrt(spread + 1e-05) * gain_ref[...]).astype(BF)
    normed_ref[...] = normed
    total = sent_ref.shape[0]
    filled = slot_tables(routes_ref[...], total, total // SLOTS)[3]
    sent_ref[...] = mm(filled.astype(F32), normed).astype(BF)


def regroup_kernel(rows_ref, out_ref):
    rows, width = out_ref.shape[1] // 2, out_ref.shape[2]
    both = rows_ref[:, 16:24].reshape(rows, width)
    for e in range(2):
        out_ref[e, :rows] = rows_ref[:, 8 * e : 8 * e + 8].reshape(rows, width)
        out_ref[e, rows:] = both


def expert_kernel(given_ref, gates_ref, down_ref, out_ref, hidden_ref, sum_ref):
    e, h = pl.program_id(0), pl.program_id(1)
    groups, _, width = out_ref.shape
    rows = groups * 8
    n = gates_ref.shape[0] * gates_ref.shape[3]
    given = given_ref[0]
    gate = dot_dims(given, gates_ref[:, 0, 0].reshape(n, width), ((1,), (1,)))
    upper = dot_dims(given, gates_ref[:, 1, 0].reshape(n, width), ((1,), (1,)))
    act = gate * jax.nn.sigmoid(gate) * upper
    r = iota(act.shape, 0)
    act = jnp.where((r < rows) | (((r & 7) >> 2) == e), act, 0.0)
    hidden_ref[:, pl.ds(pl.multiple_of(h * n, n), n)] = act.astype(BF)
    step = 512

    def finish(which):
        for k in range(0, width, step):
            at = slice(k, k + step)
            down = down_ref[:, 0, 0, :, at].reshape(hidden_ref.shape[1], step)
            out = dot_dims(hidden_ref[...], down, ((1,), (0,)))
            own = out[:rows].astype(BF).reshape(groups, 8, step)
            out_ref[:, 8 * which : 8 * which + 8, at] = own
            if which == 0:
                sum_ref[:, at] = out[rows:]
            else:
                both = (sum_ref[:, at] + out[rows:]).astype(BF)
                out_ref[:, 16:24, at] = both.reshape(groups, 8, step)

    for which in range(2):

        @pl.when((e == which) & (h == 1))
        def _():
            finish(which)


def table_kernel(routes_ref, weights_ref, out_ref):
    total = out_ref.shape[2]
    first, second, spread, filled = slot_tables(routes_ref[...], total, total // SLOTS)
    weights = weights_ref[...]
    share = 2.5 * weights / jnp.sum(weights, axis=0, keepdims=True)
    chosen = jnp.where(first, share[0:1], 0.0) + jnp.where(second, share[1:2], 0.0)
    high = chosen.astype(BF).astype(F32)
    for k, part in enumerate((high, chosen - high)):
        out_ref[k] = jnp.where(filled, mm(spread, part), 0.0).T.astype(BF)


def combine_kernel(tables_ref, results_ref, shared_ref, out_ref):
    results = results_ref[...]
    out = shared_ref[...] + (mm(tables_ref[0], results) + mm(tables_ref[1], results))
    out_ref[...] = out.astype(BF)


def project_kernel(place_ref, rows_ref, *refs):
    *blocks, out_ref = refs
    y, x, core = place_ref[0], place_ref[1], place_ref[2]
    chips = rows_ref.shape[0]
    rows = [rows_ref[z, c] for c in range(2) for z in range(chips)]
    rows = jnp.concatenate(rows, axis=0).T
    forth = jnp.where(core == 0, 3, 1)
    for down, way, ref in zip((0, 1, 3, 2), (1, 1, 3, 1), blocks):
        for right in range(4):
            at = ((y + forth * down) % 4) * 4 + (x + forth * way * (0, 1, 3, 2)[right]) % 4
            out = dot_dims(rows, ref[right], ((1,), (0,)))
            out_ref[:, pl.ds(pl.multiple_of(at * 128, 128), 128)] = out.astype(BF)


def call(kernel, out_shape, **options):
    return pl.pallas_call(
        kernel,
        out_shape=out_shape,
        compiler_params=pltpu.CompilerParams(vmem_limit_bytes=VMEM_LIMIT),
        **options,
    )


def shape(dims, dtype):
    return jax.ShapeDtypeStruct(dims, dtype)


def swap(array, axes):
    return lax.all_to_all(array, axes, split_axis=0, concat_axis=0, tiled=True)


def other_core(array):
    return lax.ppermute(array, "core", [(0, 1), (1, 0)])


def around(block, axis):
    pairs = [(2 * k, (2 * k + 2) % 8) for k in range(4)]
    pairs += [((2 * k + 3) % 8, 2 * k + 1) for k in range(4)]
    came = lax.ppermute(block, (axis, "core"), pairs)
    more = other_core(came)
    last = lax.ppermute(came, (axis, "core"), pairs)
    return [block, came, more, last]


def projection_blocks(out_weight, here):
    columns = out_weight.shape[1] // lax.axis_size(EP)
    chips = lax.axis_size("z")
    piece = lax.dynamic_slice_in_dim(out_weight, here * columns, columns, axis=1)
    heads = swap(jnp.broadcast_to(piece, (chips, *piece.shape)), "z")
    heads = heads.reshape(-1, columns)
    return heads


def shards(
    receptance,
    key_in,
    payload_vectors,
    decay_in,
    rate_in,
    gate_in,
    norm_gain,
    out_weight,
    moe_in,
    moe_gain,
    routes,
    route_weights,
    expert_gate,
    expert_up,
    expert_down,
    shared_gate,
    shared_up,
    shared_down,
):
    groups, peers = lax.axis_size(EP), lax.axis_size(TP)
    here = lax.axis_index(EP)
    length, dim = key_in.shape
    tokens, width = moe_in.shape

    local_weights = jnp.stack([w.transpose(0, 2, 1) for w in (expert_gate, expert_up, expert_down)])
    all_weights = lax.all_gather(local_weights, TP)

    core = lax.axis_index("core")
    heads = projection_blocks(out_weight, here)
    slots = expert_gate.shape[0] * SLOTS
    normed, sent = call(
        dispatch_kernel,
        (shape((tokens, width), BF), shape((groups * slots, width), BF)),
    )(moe_in, moe_gain.reshape(1, width), routes.T)
    sent, heads = lax.optimization_barrier((sent, heads))
    arrived = swap(sent.reshape(groups, slots, width), EP)
    others = other_core(heads)
    block = jnp.concatenate(
        [jnp.where(core == 0, heads, others), jnp.where(core == 0, others, heads)]
    )
    across = jnp.stack(around(block, "ep_1"))
    projection = around(across, "ep_0")

    key_in, sent = lax.optimization_barrier((key_in, sent))
    reads, total = call(
        scan_kernel, (shape((2 * dim, length), F32), shape((dim, 2 * dim), F32))
    )(key_in.T, receptance.T, payload_vectors.T, decay_in.T, rate_in.T)
    total, arrived = lax.optimization_barrier((total, arrived))
    totals = swap(jnp.broadcast_to(total, (groups, dim, 2 * dim)), EP)
    smem = pl.BlockSpec(memory_space=pltpu.SMEM)
    vmem = pl.BlockSpec(memory_space=pltpu.VMEM)
    rows = call(
        gate_kernel,
        shape((peers, dim, length // peers), BF),
        in_specs=[smem] + [vmem] * 4,
    )(here.astype(jnp.int32).reshape(1), totals, reads, gate_in.T, norm_gain.reshape(1, dim))
    token_rows = swap(rows, TP)

    gate = jnp.dot(normed, shared_gate, preferred_element_type=F32)
    upper = jnp.dot(normed, shared_up, preferred_element_type=F32)
    hidden = (jax.nn.silu(gate) * upper).astype(BF)
    shared_term = jnp.dot(hidden, shared_down, preferred_element_type=F32)

    units = expert_gate.shape[2]
    given = call(regroup_kernel, shape((2, groups * 16, width), BF))(arrived)
    tables = call(table_kernel, shape((2, tokens, groups * slots), BF))(routes.T, route_weights.T)
    results = call(
        expert_kernel,
        shape((groups, slots, width), BF),
        grid=(2, 2),
        in_specs=[
            pl.BlockSpec((1, groups * 16, width), lambda e, h: (e, 0, 0)),
            pl.BlockSpec((peers // 2, 2, 1, units, width), lambda e, h: (h, 0, e, 0, 0)),
            pl.BlockSpec((peers, 1, 1, units, width), lambda e, h: (0, 2, e, 0, 0)),
        ],
        out_specs=pl.BlockSpec((groups, slots, width), lambda e, h: (0, 0, 0)),
        scratch_shapes=[
            pltpu.VMEM((groups * 16, peers * units), BF),
            pltpu.VMEM((groups * 8, width), F32),
        ],
    )(given, all_weights, all_weights)
    results, token_rows = lax.optimization_barrier((results, token_rows))
    returned = swap(results, EP)
    moe_out = call(combine_kernel, shape((tokens, width), BF))(
        tables, returned.reshape(groups * slots, width), shared_term
    )

    place = jnp.stack([lax.axis_index(axis) for axis in EP] + [core]).astype(jnp.int32)
    mixed = call(
        project_kernel,
        shape((tokens, width), BF),
        in_specs=[smem] + [vmem] * (1 + len(projection)),
    )(place, token_rows.reshape(peers // 2, 2, dim, tokens), *projection)
    return (mixed, moe_out)


def solution(mesh):
    torus = Mesh(mesh.devices.reshape(4, 4, mesh.shape["tp"] // 2, 2), EP_TP)
    placed = (
        *(P(EP, TP),) * 6,
        P(TP),
        P(TP, None),
        P(EP_TP, None),
        P(),
        P(EP_TP, None),
        P(EP_TP, None),
        *(P(EP, None, TP),) * 3,
        P(),
        P(),
        P(),
    )

    return jax.shard_map(
        shards,
        mesh=torus,
        in_specs=placed,
        out_specs=(P(EP_TP, None), P(EP_TP, None)),
        check_vma=False,
    )
```

```python
import jax
import jax.numpy as jnp
from jax import lax
from jax.experimental import pallas as pl
from jax.experimental.pallas import tpu as pltpu
from jax.sharding import Mesh
from jax.sharding import PartitionSpec as P


CHUNK = 128
GROUP = 4
SLOTS = 12
EP = ("ep_0", "ep_1")
TP = ("z", "core")
EP_TP = EP + TP
BF = jnp.bfloat16
F32 = jnp.float32
VMEM_LIMIT = 56 * 1024 * 1024


def iota(shape, axis):
    return lax.broadcasted_iota(jnp.int32, shape, axis)


def mm(left, right):
    return jnp.dot(left.astype(BF), right.astype(BF), preferred_element_type=F32)


def mm3(left, right):
    left_high, right_high = left.astype(BF), right.astype(BF)
    left_low, right_low = left - left_high.astype(F32), right - right_high.astype(F32)
    return mm(left_high, right_high) + (mm(left_high, right_low) + mm(left_low, right_high))


def dot_dims(left, right, dims):
    return lax.dot_general(left, right, (dims, ((), ())), preferred_element_type=F32)


def scan_kernel(key_ref, recept_ref, value_ref, decay_ref, rate_ref, reads_ref, total_ref):
    dim, length = key_ref.shape
    n = CHUNK
    row, col = iota((n, n), 0), iota((n, n), 1)
    strict, inclusive = col < row, col <= row
    eye = (row == col).astype(F32)
    near = (row >> 4) == (col >> 4)
    bands = [
        ((row >> (k + 1)) == (col >> (k + 1))) & ((row >> k) != (col >> k)) for k in (4, 5, 6)
    ]
    left_half = col < dim
    upper = (row <= col).astype(BF)
    upper3 = jnp.concatenate([upper, upper, upper], axis=0)
    zero_dim = jnp.zeros((dim, n), F32)
    zero_pair = jnp.zeros((dim, 2 * n), BF)
    left_dim = iota((dim, n), 1) < dim

    def one_group(g, state):
        stage = []
        for j in range(GROUP):
            at = pl.ds(pl.multiple_of((g * GROUP + j) * n, n), n)
            keys = key_ref[:, at].astype(F32)
            recept = recept_ref[:, at].astype(F32)
            values = value_ref[:, at].astype(F32)
            unit = keys * lax.rsqrt(jnp.sum(keys * keys, axis=0, keepdims=True) + 1e-6)
            beta = unit * jax.nn.sigmoid(rate_ref[:, at].astype(F32))
            log_decay = jax.nn.sigmoid(decay_ref[:, at].astype(F32)) * (-0.6065306597126334)
            high = log_decay.astype(BF)
            rest = log_decay - high.astype(F32)
            mid = rest.astype(BF)
            low = (rest - mid.astype(F32)).astype(BF)
            cumul = jnp.dot(
                jnp.concatenate([high, mid, low], axis=1), upper3, preferred_element_type=F32
            )
            ending = cumul[:, n - 1 : n]
            grow = jnp.exp(-cumul)
            to_end = jnp.exp(ending - cumul)
            alpha_dec = -unit * jnp.exp(cumul - log_decay)
            query_dec = recept * jnp.exp(cumul)
            pair = jnp.concatenate([(beta * grow).astype(BF), (keys * grow).astype(BF)], axis=1)
            rows = jnp.concatenate([alpha_dec, query_dec], axis=0).T
            stage.append(
                dict(
                    rows=rows,
                    pair=jnp.concatenate(
                        [
                            jnp.concatenate([pair, zero_pair], axis=1),
                            jnp.concatenate([zero_pair, pair], axis=1),
                        ],
                        axis=0,
                    ),
                    value_rows=jnp.concatenate([zero_dim, values], axis=0).T,
                    beta_end=beta * to_end,
                    key_end=keys * to_end,
                    decay_all=jnp.exp(ending),
                )
            )
        for s in stage:
            scores = mm(s["rows"], s["pair"])
            s["couple"] = jnp.where(strict, scores[:, :n], 0.0)
            s["insert"] = jnp.where(strict, scores[:, n : 2 * n], 0.0)
            s["read_beta"] = jnp.where(inclusive, scores[:, 2 * n : 3 * n], 0.0)
            s["read_key"] = jnp.where(inclusive, scores[:, 3 * n :], 0.0)
        for s in stage:
            block = jnp.where(near, s["couple"], 0.0)
            s["inv"] = eye + block
            s["power"] = mm(block, block)
        for _ in range(2):
            for s in stage:
                both = mm(jnp.concatenate([s["inv"], s["power"]], axis=0), s["power"])
                s["inv"] = s["inv"] + both[:n]
                s["power"] = both[n:]
        for s in stage:
            s["inv"] = s["inv"] + mm(s["inv"], s["power"])
        for band in bands:
            for s in stage:
                s["side"] = mm(jnp.where(band, s["couple"], 0.0), s["inv"])
            for s in stage:
                s["inv"] = s["inv"] + mm(s["inv"], s["side"])
        for s in stage:
            s["through"] = mm(jnp.concatenate([s["read_beta"], s["beta_end"]], axis=0), s["inv"])
        for s in stage:
            direct = jnp.concatenate([s["read_key"], s["key_end"]], axis=0)
            s["direct"] = mm(s["through"], s["insert"]) + direct
        for s in stage:
            sources = jnp.concatenate(
                [jnp.where(left_half, s["rows"], 0.0), s["value_rows"]], axis=0
            )
            maps = mm(jnp.concatenate([s["through"], s["direct"]], axis=1), sources)
            query = jnp.where(left_half, pltpu.roll(s["rows"], dim, 1), 0.0)
            s["reads"] = maps[:n] + query
            s["moves"] = maps[n:]
        for j, s in enumerate(stage):
            at = pl.ds(pl.multiple_of((g * GROUP + j) * n, n), n)
            left = jnp.concatenate([s["reads"], s["moves"]], axis=0)[:, :dim]
            met = mm(left, state)
            out = met[:n] + jnp.where(left_half, 0.0, s["reads"])
            reads_ref[:, at] = out.T
            state = s["decay_all"] * state + met[n:] + jnp.where(left_dim, 0.0, s["moves"])
        return state

    start = (iota((dim, n), 0) == iota((dim, n), 1)).astype(F32)
    total_ref[...] = lax.fori_loop(0, length // (n * GROUP), one_group, start)


def gate_kernel(here_ref, totals_ref, reads_ref, gate_ref, gain_ref, out_ref):
    dim = gate_ref.shape[0]
    right = iota((dim, 2 * dim), 1) >= dim

    def pass_device(d, entry):
        total = totals_ref[d]
        moved = mm3(total[:, :dim], entry)
        return jnp.where(right, moved + total, 0.0)

    entry = lax.fori_loop(0, here_ref[0], pass_device, jnp.zeros((dim, 2 * dim), F32))
    entry = jnp.concatenate([entry, jnp.zeros_like(entry)], axis=0).T[dim:, :dim]
    gain = jnp.broadcast_to(gain_ref[...], (dim, dim))
    same = iota((dim, dim), 0) == iota((dim, dim), 1)
    gain = jnp.sum(jnp.where(same, gain, 0.0), axis=1, keepdims=True)
    parts = out_ref.shape[0]
    n = out_ref.shape[2]
    step = 4

    for j in range(0, parts, step):
        at = slice(j * n, (j + step) * n)
        recur = mm(entry, reads_ref[:dim, at]) + reads_ref[dim:, at]
        centered = recur - jnp.mean(recur, axis=0, keepdims=True)
        spread = jnp.mean(centered * centered, axis=0, keepdims=True)
        normed = centered * lax.rsqrt(spread + 0.00064)
        gated = normed * gain * jax.nn.sigmoid(gate_ref[:, at].astype(F32))
        for k in range(step):
            out_ref[j + k] = gated[:, k * n : (k + 1) * n].astype(BF)


def slot_tables(routes, total, experts):
    tokens = routes.shape[1]
    expert = iota((experts, tokens), 0)
    first, second = routes[0:1] == expert, routes[1:2] == expert
    picked = first | second
    before = (iota((tokens, tokens), 0) < iota((tokens, tokens), 1)).astype(BF)
    rank = mm(picked.astype(F32), before)
    marked = jnp.where(picked, rank + 1.0, 0.0)

    def places(shape):
        r = iota(shape, 0)
        group = (r * 2731) >> 16
        q = r - group * 24
        odd = ((q >= 8) & (q < 16)) | (q >= 20)
        base = jnp.where(q < 8, 0, jnp.where(q < 16, 8, jnp.where(q < 20, 8, 12)))
        return group * 2 + odd.astype(jnp.int32), q - base

    owner, unused = places((total, experts))
    spread = (owner == iota((total, experts), 1)).astype(F32)
    unused, place = places((total, tokens))
    filled = mm(spread, marked) == (place + 1).astype(F32)
    return first, second, spread, filled


def dispatch_kernel(moe_ref, gain_ref, routes_ref, normed_ref, sent_ref):
    values = moe_ref[...].astype(F32)
    centered = values - jnp.mean(values, axis=1, keepdims=True)
    spread = jnp.mean(centered * centered, axis=1, keepdims=True)
    normed = (centered * lax.rsqrt(spread + 1e-05) * gain_ref[...]).astype(BF)
    normed_ref[...] = normed
    total = sent_ref.shape[0]
    filled = slot_tables(routes_ref[...], total, total // SLOTS)[3]
    sent_ref[...] = mm(filled.astype(F32), normed).astype(BF)


def regroup_kernel(rows_ref, out_ref):
    rows, width = out_ref.shape[1] // 2, out_ref.shape[2]
    both = rows_ref[:, 16:24].reshape(rows, width)
    for e in range(2):
        out_ref[e, :rows] = rows_ref[:, 8 * e : 8 * e + 8].reshape(rows, width)
        out_ref[e, rows:] = both


def expert_kernel(given_ref, gates_ref, weights_ref, out_ref, down_ref, hidden_ref, sum_ref, sems):
    e, h = pl.program_id(0), pl.program_id(1)
    groups, _, width = out_ref.shape
    rows = groups * 8
    n = gates_ref.shape[0] * gates_ref.shape[3]

    def down_copy(which):
        source = weights_ref.at[:, 2, which]
        return pltpu.make_async_copy(source, down_ref.at[which], sems.at[which])

    @pl.when((e == 0) & (h == 0))
    def _():
        down_copy(0).start()
        down_copy(1).start()

    given = given_ref[0]
    gate = dot_dims(given, gates_ref[:, 0, 0].reshape(n, width), ((1,), (1,)))
    upper = dot_dims(given, gates_ref[:, 1, 0].reshape(n, width), ((1,), (1,)))
    act = gate * jax.nn.sigmoid(gate) * upper
    r = iota(act.shape, 0)
    act = jnp.where((r < rows) | (((r & 7) >> 2) == e), act, 0.0)
    hidden_ref[:, pl.ds(pl.multiple_of(h * n, n), n)] = act.astype(BF)
    step = 512

    def finish(which):
        down_copy(which).wait()
        for k in range(0, width, step):
            at = slice(k, k + step)
            down = down_ref[which, :, :, at].reshape(hidden_ref.shape[1], step)
            out = dot_dims(hidden_ref[...], down, ((1,), (0,)))
            own = out[:rows].astype(BF).reshape(groups, 8, step)
            out_ref[:, 8 * which : 8 * which + 8, at] = own
            if which == 0:
                sum_ref[:, at] = out[rows:]
            else:
                both = (sum_ref[:, at] + out[rows:]).astype(BF)
                out_ref[:, 16:24, at] = both.reshape(groups, 8, step)

    for which in range(2):

        @pl.when((e == which) & (h == 1))
        def _():
            finish(which)


def table_kernel(routes_ref, weights_ref, out_ref):
    total = out_ref.shape[2]
    first, second, spread, filled = slot_tables(routes_ref[...], total, total // SLOTS)
    weights = weights_ref[...]
    share = 2.5 * weights / jnp.sum(weights, axis=0, keepdims=True)
    chosen = jnp.where(first, share[0:1], 0.0) + jnp.where(second, share[1:2], 0.0)
    high = chosen.astype(BF).astype(F32)
    for k, part in enumerate((high, chosen - high)):
        out_ref[k] = jnp.where(filled, mm(spread, part), 0.0).T.astype(BF)


def combine_kernel(tables_ref, results_ref, shared_ref, out_ref):
    results = results_ref[...]
    out = shared_ref[...] + (mm(tables_ref[0], results) + mm(tables_ref[1], results))
    out_ref[...] = out.astype(BF)


def project_kernel(place_ref, rows_ref, *refs):
    *blocks, out_ref = refs
    y, x, core = place_ref[0], place_ref[1], place_ref[2]
    chips = rows_ref.shape[0]
    rows = [rows_ref[z, c] for c in range(2) for z in range(chips)]
    rows = jnp.concatenate(rows, axis=0).T
    forth = jnp.where(core == 0, 3, 1)
    for down, way, ref in zip((0, 1, 3, 2), (1, 1, 3, 1), blocks):
        for right in range(4):
            at = ((y + forth * down) % 4) * 4 + (x + forth * way * (0, 1, 3, 2)[right]) % 4
            out = dot_dims(rows, ref[right], ((1,), (0,)))
            out_ref[:, pl.ds(pl.multiple_of(at * 128, 128), 128)] = out.astype(BF)


def call(kernel, out_shape, **options):
    return pl.pallas_call(
        kernel,
        out_shape=out_shape,
        compiler_params=pltpu.CompilerParams(vmem_limit_bytes=VMEM_LIMIT),
        **options,
    )


def shape(dims, dtype):
    return jax.ShapeDtypeStruct(dims, dtype)


def swap(array, axes):
    return lax.all_to_all(array, axes, split_axis=0, concat_axis=0, tiled=True)


def other_core(array):
    return lax.ppermute(array, "core", [(0, 1), (1, 0)])


def around(block, axis):
    pairs = [(2 * k, (2 * k + 2) % 8) for k in range(4)]
    pairs += [((2 * k + 3) % 8, 2 * k + 1) for k in range(4)]
    came = lax.ppermute(block, (axis, "core"), pairs)
    more = other_core(came)
    last = lax.ppermute(came, (axis, "core"), pairs)
    return [block, came, more, last]


def projection_blocks(out_weight, here):
    columns = out_weight.shape[1] // lax.axis_size(EP)
    chips = lax.axis_size("z")
    piece = lax.dynamic_slice_in_dim(out_weight, here * columns, columns, axis=1)
    heads = swap(jnp.broadcast_to(piece, (chips, *piece.shape)), "z")
    heads = heads.reshape(-1, columns)
    return heads


def shards(
    receptance,
    key_in,
    payload_vectors,
    decay_in,
    rate_in,
    gate_in,
    norm_gain,
    out_weight,
    moe_in,
    moe_gain,
    routes,
    route_weights,
    expert_gate,
    expert_up,
    expert_down,
    shared_gate,
    shared_up,
    shared_down,
):
    groups, peers = lax.axis_size(EP), lax.axis_size(TP)
    here = lax.axis_index(EP)
    length, dim = key_in.shape
    tokens, width = moe_in.shape

    local_weights = jnp.stack([w.transpose(0, 2, 1) for w in (expert_gate, expert_up, expert_down)])
    all_weights = lax.all_gather(local_weights, TP)

    core = lax.axis_index("core")
    heads = projection_blocks(out_weight, here)
    slots = expert_gate.shape[0] * SLOTS
    normed, sent = call(
        dispatch_kernel,
        (shape((tokens, width), BF), shape((groups * slots, width), BF)),
    )(moe_in, moe_gain.reshape(1, width), routes.T)
    sent, heads = lax.optimization_barrier((sent, heads))
    arrived = swap(sent.reshape(groups, slots, width), EP)
    others = other_core(heads)
    block = jnp.concatenate(
        [jnp.where(core == 0, heads, others), jnp.where(core == 0, others, heads)]
    )
    across = jnp.stack(around(block, "ep_1"))
    projection = around(across, "ep_0")

    key_in, sent = lax.optimization_barrier((key_in, sent))
    reads, total = call(
        scan_kernel, (shape((2 * dim, length), F32), shape((dim, 2 * dim), F32))
    )(key_in.T, receptance.T, payload_vectors.T, decay_in.T, rate_in.T)
    total, arrived = lax.optimization_barrier((total, arrived))
    totals = swap(jnp.broadcast_to(total, (groups, dim, 2 * dim)), EP)
    smem = pl.BlockSpec(memory_space=pltpu.SMEM)
    vmem = pl.BlockSpec(memory_space=pltpu.VMEM)
    rows = call(
        gate_kernel,
        shape((peers, dim, length // peers), BF),
        in_specs=[smem] + [vmem] * 4,
    )(here.astype(jnp.int32).reshape(1), totals, reads, gate_in.T, norm_gain.reshape(1, dim))
    token_rows = swap(rows, TP)

    gate = jnp.dot(normed, shared_gate, preferred_element_type=F32)
    upper = jnp.dot(normed, shared_up, preferred_element_type=F32)
    hidden = (jax.nn.silu(gate) * upper).astype(BF)
    shared_term = jnp.dot(hidden, shared_down, preferred_element_type=F32)

    units = expert_gate.shape[2]
    given = call(regroup_kernel, shape((2, groups * 16, width), BF))(arrived)
    tables = call(table_kernel, shape((2, tokens, groups * slots), BF))(routes.T, route_weights.T)
    results = call(
        expert_kernel,
        shape((groups, slots, width), BF),
        grid=(2, 2),
        in_specs=[
            pl.BlockSpec((1, groups * 16, width), lambda e, h: (e, 0, 0)),
            pl.BlockSpec((peers // 2, 2, 1, units, width), lambda e, h: (h, 0, e, 0, 0)),
            pl.BlockSpec(memory_space=pl.ANY),
        ],
        out_specs=pl.BlockSpec((groups, slots, width), lambda e, h: (0, 0, 0)),
        scratch_shapes=[
            pltpu.VMEM((2, peers, units, width), BF),
            pltpu.VMEM((groups * 16, peers * units), BF),
            pltpu.VMEM((groups * 8, width), F32),
            pltpu.SemaphoreType.DMA((2,)),
        ],
    )(given, all_weights, all_weights)
    results, token_rows = lax.optimization_barrier((results, token_rows))
    returned = swap(results, EP)
    moe_out = call(combine_kernel, shape((tokens, width), BF))(
        tables, returned.reshape(groups * slots, width), shared_term
    )

    place = jnp.stack([lax.axis_index(axis) for axis in EP] + [core]).astype(jnp.int32)
    mixed = call(
        project_kernel,
        shape((tokens, width), BF),
        in_specs=[smem] + [vmem] * (1 + len(projection)),
    )(place, token_rows.reshape(peers // 2, 2, dim, tokens), *projection)
    return (mixed, moe_out)


def solution(mesh):
    torus = Mesh(mesh.devices.reshape(4, 4, mesh.shape["tp"] // 2, 2), EP_TP)
    placed = (
        *(P(EP, TP),) * 6,
        P(TP),
        P(TP, None),
        P(EP_TP, None),
        P(),
        P(EP_TP, None),
        P(EP_TP, None),
        *(P(EP, None, TP),) * 3,
        P(),
        P(),
        P(),
    )

    return jax.shard_map(
        shards,
        mesh=torus,
        in_specs=placed,
        out_specs=(P(EP_TP, None), P(EP_TP, None)),
        check_vma=False,
    )
```

```python
import jax
import jax.numpy as jnp
from jax import lax
from jax.experimental import pallas as pl
from jax.experimental.pallas import tpu as pltpu
from jax.sharding import Mesh
from jax.sharding import PartitionSpec as P


CHUNK = 128
GROUP = 4
SLOTS = 12
EP = ("ep_0", "ep_1")
TP = ("z", "core")
EP_TP = EP + TP
BF = jnp.bfloat16
F32 = jnp.float32
VMEM_LIMIT = 56 * 1024 * 1024


def iota(shape, axis):
    return lax.broadcasted_iota(jnp.int32, shape, axis)


def mm(left, right):
    return jnp.dot(left.astype(BF), right.astype(BF), preferred_element_type=F32)


def mm3(left, right):
    left_high, right_high = left.astype(BF), right.astype(BF)
    left_low, right_low = left - left_high.astype(F32), right - right_high.astype(F32)
    return mm(left_high, right_high) + (mm(left_high, right_low) + mm(left_low, right_high))


def dot_dims(left, right, dims):
    return lax.dot_general(left, right, (dims, ((), ())), preferred_element_type=F32)


def scan_kernel(key_ref, recept_ref, value_ref, decay_ref, rate_ref, reads_ref, total_ref):
    dim, length = key_ref.shape
    n = CHUNK
    row, col = iota((n, n), 0), iota((n, n), 1)
    strict, inclusive = col < row, col <= row
    eye = (row == col).astype(F32)
    near = (row >> 4) == (col >> 4)
    bands = [
        ((row >> (k + 1)) == (col >> (k + 1))) & ((row >> k) != (col >> k)) for k in (4, 5, 6)
    ]
    left_half = col < dim
    upper = (row <= col).astype(BF)
    upper3 = jnp.concatenate([upper, upper, upper], axis=0)
    zero_dim = jnp.zeros((dim, n), F32)
    zero_pair = jnp.zeros((dim, 2 * n), BF)
    left_dim = iota((dim, n), 1) < dim

    def one_group(g, state):
        stage = []
        for j in range(GROUP):
            at = pl.ds(pl.multiple_of((g * GROUP + j) * n, n), n)
            keys = key_ref[:, at].astype(F32)
            recept = recept_ref[:, at].astype(F32)
            values = value_ref[:, at].astype(F32)
            unit = keys * lax.rsqrt(jnp.sum(keys * keys, axis=0, keepdims=True) + 1e-6)
            beta = unit * jax.nn.sigmoid(rate_ref[:, at].astype(F32))
            log_decay = jax.nn.sigmoid(decay_ref[:, at].astype(F32)) * (-0.6065306597126334)
            high = log_decay.astype(BF)
            rest = log_decay - high.astype(F32)
            mid = rest.astype(BF)
            low = (rest - mid.astype(F32)).astype(BF)
            cumul = jnp.dot(
                jnp.concatenate([high, mid, low], axis=1), upper3, preferred_element_type=F32
            )
            ending = cumul[:, n - 1 : n]
            grow = jnp.exp(-cumul)
            to_end = jnp.exp(ending - cumul)
            alpha_dec = -unit * jnp.exp(cumul - log_decay)
            query_dec = recept * jnp.exp(cumul)
            pair = jnp.concatenate([(beta * grow).astype(BF), (keys * grow).astype(BF)], axis=1)
            rows = jnp.concatenate([alpha_dec, query_dec], axis=0).T
            stage.append(
                dict(
                    rows=rows,
                    pair=jnp.concatenate(
                        [
                            jnp.concatenate([pair, zero_pair], axis=1),
                            jnp.concatenate([zero_pair, pair], axis=1),
                        ],
                        axis=0,
                    ),
                    value_rows=jnp.concatenate([zero_dim, values], axis=0).T,
                    beta_end=beta * to_end,
                    key_end=keys * to_end,
                    decay_all=jnp.exp(ending),
                )
            )
        for s in stage:
            scores = mm(s["rows"], s["pair"])
            s["couple"] = jnp.where(strict, scores[:, :n], 0.0)
            s["insert"] = jnp.where(strict, scores[:, n : 2 * n], 0.0)
            s["read_beta"] = jnp.where(inclusive, scores[:, 2 * n : 3 * n], 0.0)
            s["read_key"] = jnp.where(inclusive, scores[:, 3 * n :], 0.0)
        for s in stage:
            block = jnp.where(near, s["couple"], 0.0)
            s["inv"] = eye + block
            s["power"] = mm(block, block)
        for _ in range(2):
            for s in stage:
                both = mm(jnp.concatenate([s["inv"], s["power"]], axis=0), s["power"])
                s["inv"] = s["inv"] + both[:n]
                s["power"] = both[n:]
        for s in stage:
            s["inv"] = s["inv"] + mm(s["inv"], s["power"])
        for band in bands:
            for s in stage:
                s["side"] = mm(jnp.where(band, s["couple"], 0.0), s["inv"])
            for s in stage:
                s["inv"] = s["inv"] + mm(s["inv"], s["side"])
        for s in stage:
            s["through"] = mm(jnp.concatenate([s["read_beta"], s["beta_end"]], axis=0), s["inv"])
        for s in stage:
            direct = jnp.concatenate([s["read_key"], s["key_end"]], axis=0)
            s["direct"] = mm(s["through"], s["insert"]) + direct
        for s in stage:
            sources = jnp.concatenate(
                [jnp.where(left_half, s["rows"], 0.0), s["value_rows"]], axis=0
            )
            maps = mm(jnp.concatenate([s["through"], s["direct"]], axis=1), sources)
            query = jnp.where(left_half, pltpu.roll(s["rows"], dim, 1), 0.0)
            s["reads"] = maps[:n] + query
            s["moves"] = maps[n:]
        for j, s in enumerate(stage):
            at = pl.ds(pl.multiple_of((g * GROUP + j) * n, n), n)
            left = jnp.concatenate([s["reads"], s["moves"]], axis=0)[:, :dim]
            met = mm(left, state)
            out = met[:n] + jnp.where(left_half, 0.0, s["reads"])
            reads_ref[:, at] = out.T
            state = s["decay_all"] * state + met[n:] + jnp.where(left_dim, 0.0, s["moves"])
        return state

    start = (iota((dim, n), 0) == iota((dim, n), 1)).astype(F32)
    total_ref[...] = lax.fori_loop(0, length // (n * GROUP), one_group, start)


def gate_kernel(here_ref, totals_ref, reads_ref, gate_ref, gain_ref, out_ref):
    dim = gate_ref.shape[0]
    right = iota((dim, 2 * dim), 1) >= dim

    def pass_device(d, entry):
        total = totals_ref[d]
        moved = mm3(total[:, :dim], entry)
        return jnp.where(right, moved + total, 0.0)

    entry = lax.fori_loop(0, here_ref[0], pass_device, jnp.zeros((dim, 2 * dim), F32))
    entry = jnp.concatenate([entry, jnp.zeros_like(entry)], axis=0).T[dim:, :dim]
    gain = jnp.broadcast_to(gain_ref[...], (dim, dim))
    same = iota((dim, dim), 0) == iota((dim, dim), 1)
    gain = jnp.sum(jnp.where(same, gain, 0.0), axis=1, keepdims=True)
    parts = out_ref.shape[0]
    n = out_ref.shape[2]
    step = 4

    for j in range(0, parts, step):
        at = slice(j * n, (j + step) * n)
        recur = mm(entry, reads_ref[:dim, at]) + reads_ref[dim:, at]
        centered = recur - jnp.mean(recur, axis=0, keepdims=True)
        spread = jnp.mean(centered * centered, axis=0, keepdims=True)
        normed = centered * lax.rsqrt(spread + 0.00064)
        gated = normed * gain * jax.nn.sigmoid(gate_ref[:, at].astype(F32))
        for k in range(step):
            out_ref[j + k] = gated[:, k * n : (k + 1) * n].astype(BF)


def slot_tables(routes, total, experts):
    tokens = routes.shape[1]
    expert = iota((experts, tokens), 0)
    first, second = routes[0:1] == expert, routes[1:2] == expert
    picked = first | second
    before = (iota((tokens, tokens), 0) < iota((tokens, tokens), 1)).astype(BF)
    rank = mm(picked.astype(F32), before)
    marked = jnp.where(picked, rank + 1.0, 0.0)

    def places(shape):
        r = iota(shape, 0)
        group = (r * 2731) >> 16
        q = r - group * 24
        odd = ((q >= 8) & (q < 16)) | (q >= 20)
        base = jnp.where(q < 8, 0, jnp.where(q < 16, 8, jnp.where(q < 20, 8, 12)))
        return group * 2 + odd.astype(jnp.int32), q - base

    owner, unused = places((total, experts))
    spread = (owner == iota((total, experts), 1)).astype(F32)
    unused, place = places((total, tokens))
    filled = mm(spread, marked) == (place + 1).astype(F32)
    return first, second, spread, filled


def dispatch_kernel(moe_ref, gain_ref, routes_ref, normed_ref, sent_ref):
    values = moe_ref[...].astype(F32)
    centered = values - jnp.mean(values, axis=1, keepdims=True)
    spread = jnp.mean(centered * centered, axis=1, keepdims=True)
    normed = (centered * lax.rsqrt(spread + 1e-05) * gain_ref[...]).astype(BF)
    normed_ref[...] = normed
    total = sent_ref.shape[0]
    filled = slot_tables(routes_ref[...], total, total // SLOTS)[3]
    sent_ref[...] = mm(filled.astype(F32), normed).astype(BF)


def pack_kernel(first_ref, second_ref, third_ref, out_ref, sems):
    copies = [
        pltpu.make_async_copy(ref, out_ref.at[k], sems.at[k])
        for k, ref in enumerate((first_ref, second_ref, third_ref))
    ]
    for copy in copies:
        copy.start()
    for copy in copies:
        copy.wait()


def regroup_kernel(rows_ref, out_ref):
    rows, width = out_ref.shape[1] // 2, out_ref.shape[2]
    both = rows_ref[:, 16:24].reshape(rows, width)
    for e in range(2):
        out_ref[e, :rows] = rows_ref[:, 8 * e : 8 * e + 8].reshape(rows, width)
        out_ref[e, rows:] = both


def expert_kernel(given_ref, gates_ref, weights_ref, out_ref, down_ref, hidden_ref, sum_ref, sems):
    e, h = pl.program_id(0), pl.program_id(1)
    groups, _, width = out_ref.shape
    rows = groups * 8
    n = gates_ref.shape[0] * gates_ref.shape[3]

    def down_copy(which):
        source = weights_ref.at[:, 2, which]
        return pltpu.make_async_copy(source, down_ref.at[which], sems.at[which])

    @pl.when((e == 0) & (h == 0))
    def _():
        down_copy(0).start()
        down_copy(1).start()

    given = given_ref[0]
    gate = dot_dims(given, gates_ref[:, 0, 0].reshape(n, width), ((1,), (1,)))
    upper = dot_dims(given, gates_ref[:, 1, 0].reshape(n, width), ((1,), (1,)))
    act = gate * jax.nn.sigmoid(gate) * upper
    r = iota(act.shape, 0)
    act = jnp.where((r < rows) | (((r & 7) >> 2) == e), act, 0.0)
    hidden_ref[:, pl.ds(pl.multiple_of(h * n, n), n)] = act.astype(BF)
    step = 512

    def finish(which):
        down_copy(which).wait()
        for k in range(0, width, step):
            at = slice(k, k + step)
            down = down_ref[which, :, :, at].reshape(hidden_ref.shape[1], step)
            out = dot_dims(hidden_ref[...], down, ((1,), (0,)))
            own = out[:rows].astype(BF).reshape(groups, 8, step)
            out_ref[:, 8 * which : 8 * which + 8, at] = own
            if which == 0:
                sum_ref[:, at] = out[rows:]
            else:
                both = (sum_ref[:, at] + out[rows:]).astype(BF)
                out_ref[:, 16:24, at] = both.reshape(groups, 8, step)

    for which in range(2):

        @pl.when((e == which) & (h == 1))
        def _():
            finish(which)


def table_kernel(routes_ref, weights_ref, out_ref):
    total = out_ref.shape[2]
    first, second, spread, filled = slot_tables(routes_ref[...], total, total // SLOTS)
    weights = weights_ref[...]
    share = 2.5 * weights / jnp.sum(weights, axis=0, keepdims=True)
    chosen = jnp.where(first, share[0:1], 0.0) + jnp.where(second, share[1:2], 0.0)
    high = chosen.astype(BF).astype(F32)
    for k, part in enumerate((high, chosen - high)):
        out_ref[k] = jnp.where(filled, mm(spread, part), 0.0).T.astype(BF)


def combine_kernel(tables_ref, results_ref, shared_ref, out_ref):
    step = 512
    for k in range(0, out_ref.shape[1], step):
        at = slice(k, k + step)
        results = results_ref[:, at]
        out = shared_ref[:, at] + (mm(tables_ref[0], results) + mm(tables_ref[1], results))
        out_ref[:, at] = out.astype(BF)


def project_kernel(place_ref, rows_ref, *refs):
    *blocks, out_ref = refs
    y, x, core = place_ref[0], place_ref[1], place_ref[2]
    chips = rows_ref.shape[0]
    rows = [rows_ref[z, c] for c in range(2) for z in range(chips)]
    rows = jnp.concatenate(rows, axis=0).T
    forth = jnp.where(core == 0, 3, 1)
    for down, way, ref in zip((0, 1, 3, 2), (1, 1, 3, 1), blocks):
        for right in range(4):
            at = ((y + forth * down) % 4) * 4 + (x + forth * way * (0, 1, 3, 2)[right]) % 4
            out = dot_dims(rows, ref[right], ((1,), (0,)))
            out_ref[:, pl.ds(pl.multiple_of(at * 128, 128), 128)] = out.astype(BF)


def call(kernel, out_shape, **options):
    return pl.pallas_call(
        kernel,
        out_shape=out_shape,
        compiler_params=pltpu.CompilerParams(vmem_limit_bytes=VMEM_LIMIT),
        **options,
    )


def shape(dims, dtype):
    return jax.ShapeDtypeStruct(dims, dtype)


def swap(array, axes):
    return lax.all_to_all(array, axes, split_axis=0, concat_axis=0, tiled=True)


def other_core(array):
    return lax.ppermute(array, "core", [(0, 1), (1, 0)])


def around(block, axis):
    pairs = [(2 * k, (2 * k + 2) % 8) for k in range(4)]
    pairs += [((2 * k + 3) % 8, 2 * k + 1) for k in range(4)]
    came = lax.ppermute(block, (axis, "core"), pairs)
    more = other_core(came)
    last = lax.ppermute(came, (axis, "core"), pairs)
    return [block, came, more, last]


def projection_blocks(out_weight, here):
    columns = out_weight.shape[1] // lax.axis_size(EP)
    chips = lax.axis_size("z")
    piece = lax.dynamic_slice_in_dim(out_weight, here * columns, columns, axis=1)
    heads = swap(jnp.broadcast_to(piece, (chips, *piece.shape)), "z")
    heads = heads.reshape(-1, columns)
    return heads


def shards(
    receptance,
    key_in,
    payload_vectors,
    decay_in,
    rate_in,
    gate_in,
    norm_gain,
    out_weight,
    moe_in,
    moe_gain,
    routes,
    route_weights,
    expert_gate,
    expert_up,
    expert_down,
    shared_gate,
    shared_up,
    shared_down,
):
    groups, peers = lax.axis_size(EP), lax.axis_size(TP)
    here = lax.axis_index(EP)
    length, dim = key_in.shape
    tokens, width = moe_in.shape

    weights = [w.transpose(0, 2, 1) for w in (expert_gate, expert_up, expert_down)]
    hbm = pl.BlockSpec(memory_space=pl.ANY)
    local_weights = call(
        pack_kernel,
        shape((3, *weights[0].shape), BF),
        in_specs=[hbm] * 3,
        out_specs=hbm,
        scratch_shapes=[pltpu.SemaphoreType.DMA((3,))],
    )(*weights)
    all_weights = lax.all_gather(local_weights, TP)

    core = lax.axis_index("core")
    heads = projection_blocks(out_weight, here)
    slots = expert_gate.shape[0] * SLOTS
    normed, sent = call(
        dispatch_kernel,
        (shape((tokens, width), BF), shape((groups * slots, width), BF)),
    )(moe_in, moe_gain.reshape(1, width), routes.T)
    sent, heads = lax.optimization_barrier((sent, heads))
    arrived = swap(sent.reshape(groups, slots, width), EP)
    others = other_core(heads)
    block = jnp.concatenate(
        [jnp.where(core == 0, heads, others), jnp.where(core == 0, others, heads)]
    )
    across = jnp.stack(around(block, "ep_1"))
    projection = around(across, "ep_0")

    key_in, sent = lax.optimization_barrier((key_in, sent))
    reads, total = call(
        scan_kernel, (shape((2 * dim, length), F32), shape((dim, 2 * dim), F32))
    )(key_in.T, receptance.T, payload_vectors.T, decay_in.T, rate_in.T)
    total, arrived = lax.optimization_barrier((total, arrived))
    totals = swap(jnp.broadcast_to(total, (groups, dim, 2 * dim)), EP)
    smem = pl.BlockSpec(memory_space=pltpu.SMEM)
    vmem = pl.BlockSpec(memory_space=pltpu.VMEM)
    rows = call(
        gate_kernel,
        shape((peers, dim, length // peers), BF),
        in_specs=[smem] + [vmem] * 4,
    )(here.astype(jnp.int32).reshape(1), totals, reads, gate_in.T, norm_gain.reshape(1, dim))
    token_rows = swap(rows, TP)

    gate = jnp.dot(normed, shared_gate, preferred_element_type=F32)
    upper = jnp.dot(normed, shared_up, preferred_element_type=F32)
    hidden = (jax.nn.silu(gate) * upper).astype(BF)
    shared_term = jnp.dot(hidden, shared_down, preferred_element_type=F32)

    units = expert_gate.shape[2]
    given = call(regroup_kernel, shape((2, groups * 16, width), BF))(arrived)
    tables = call(table_kernel, shape((2, tokens, groups * slots), BF))(routes.T, route_weights.T)
    results = call(
        expert_kernel,
        shape((groups, slots, width), BF),
        grid=(2, 2),
        in_specs=[
            pl.BlockSpec((1, groups * 16, width), lambda e, h: (e, 0, 0)),
            pl.BlockSpec((peers // 2, 2, 1, units, width), lambda e, h: (h, 0, e, 0, 0)),
            pl.BlockSpec(memory_space=pl.ANY),
        ],
        out_specs=pl.BlockSpec((groups, slots, width), lambda e, h: (0, 0, 0)),
        scratch_shapes=[
            pltpu.VMEM((2, peers, units, width), BF),
            pltpu.VMEM((groups * 16, peers * units), BF),
            pltpu.VMEM((groups * 8, width), F32),
            pltpu.SemaphoreType.DMA((2,)),
        ],
    )(given, all_weights, all_weights)
    results, token_rows = lax.optimization_barrier((results, token_rows))
    returned = swap(results, EP)
    moe_out = call(combine_kernel, shape((tokens, width), BF))(
        tables, returned.reshape(groups * slots, width), shared_term
    )

    place = jnp.stack([lax.axis_index(axis) for axis in EP] + [core]).astype(jnp.int32)
    mixed = call(
        project_kernel,
        shape((tokens, width), BF),
        in_specs=[smem] + [vmem] * (1 + len(projection)),
    )(place, token_rows.reshape(peers // 2, 2, dim, tokens), *projection)
    return (mixed, moe_out)


def solution(mesh):
    torus = Mesh(mesh.devices.reshape(4, 4, mesh.shape["tp"] // 2, 2), EP_TP)
    placed = (
        *(P(EP, TP),) * 6,
        P(TP),
        P(TP, None),
        P(EP_TP, None),
        P(),
        P(EP_TP, None),
        P(EP_TP, None),
        *(P(EP, None, TP),) * 3,
        P(),
        P(),
        P(),
    )

    return jax.shard_map(
        shards,
        mesh=torus,
        in_specs=placed,
        out_specs=(P(EP_TP, None), P(EP_TP, None)),
        check_vma=False,
    )
```
